256 devices in a mesh: sp: 64 (over z, y, core), tp: 4 (over x).
Axes of the slice: x: 4, y: 4, z: 8, core: 2. Of those that a mesh axis runs over, the one named last changes fastest.
Arguments:
- resid: bfloat16 [24576, 2048], P(('sp', 'tp')), may hold values from -6 to 6
- conv_b: bfloat16 [24576, 1024], P('sp', 'tp'), may hold values from -6 to 6
- conv_c: bfloat16 [24576, 1024], P('sp', 'tp'), may hold values from -6 to 6
- conv_x: bfloat16 [24576, 1024], P('sp', 'tp'), may hold values from -6 to 6
- conv_taps: bfloat16 [3, 1024], P(None, 'tp'), may hold values from -3.5 to 3.5
- out_weight: bfloat16 [1024, 2048], P('tp'), may hold values from -0.1875 to 0.1875
- norm_gain: float32 [2048], replicated, may hold values from 0.1 to 1.9
- routes: int32 [24576, 2], P('sp'), may hold values from 0 to 63, all different within a row; in each aligned block of 96 rows (0 to 95, 96 to 191, ...) at most 4 rows name the same one
- route_weight: float32 [24576, 2], P('sp'), may hold values from 0.2 to 1
- expert_gate: bfloat16 [64, 2048, 1024], P('sp', None, 'tp'), may hold values from -0.125 to 0.125
- expert_up: bfloat16 [64, 2048, 1024], P('sp', None, 'tp'), may hold values from -0.125 to 0.125
- expert_down: bfloat16 [64, 1024, 2048], P('sp', 'tp'), may hold values from -0.1875 to 0.1875
- shared_gate: bfloat16 [2048, 1024], P(None, 'tp'), may hold values from -0.125 to 0.125
- shared_up: bfloat16 [2048, 1024], P(None, 'tp'), may hold values from -0.125 to 0.125
- shared_down: bfloat16 [1024, 2048], P('tp'), may hold values from -0.1875 to 0.1875
Outputs:
- layer_out: bfloat16 [24576, 2048], P(('sp', 'tp'))
The draws below stay inside these ranges and needn't reach their ends.
Inputs may be any that keep to these rules, and one draw needn't show every extreme that they name: `routes`: in each aligned block of 96 tokens no expert is named more than 4 times; in some blocks some expert is named exactly 4 times; each row names 2 different experts.
All inputs are finite; a program needn't handle non-finite values.
Results may differ from the reference program's by a relative error of at most 0.015.
Values may be sent and summed in bfloat16 or wider, within the bound.
A program may use at most 128 MiB of HBM per device.

```python
import math
import jax
import jax.numpy as jnp
import numpy as np
from jax import lax

D = 2048
CONV = 1024
FF_E = 1024
TAPS = 3
TOP_K = 2
TOK_DEV = 384
TOKENS = 24576
EXPERTS = 64
CAP = 4
N_TP = 4


def levels(stream_key, shape, pieces, smallest, top_value):
    def one(dim, parts):
        draws = jax.random.uniform(jax.random.fold_in(jax.random.fold_in(stream_key, 6), dim), (parts,), jnp.float32, smallest / len(pieces), top_value / len(pieces))
        return jnp.repeat(jnp.exp(draws), shape[dim] // parts).reshape((-1,) + (1,) * (len(shape) - dim - 1))

    gain = one(*pieces[0])
    for cut in pieces[1:]:
        gain = gain * one(*cut)
    return gain


def shared_out(key, own, number, rows, amount, top, bound, skew):
    sequence = jax.random.permutation(key, amount)
    packed, common = portions_of(amount, rows * top, bound, skew, True), portions_of(amount, rows * top, bound, skew, False)
    places = jnp.arange(amount)

    def named(tallies, turn):
        used = int((tallies > 0).sum())
        fixed = max(1, used // 4)
        passed = fixed + (places - fixed + turn * (used - fixed)) % max(1, amount - fixed)
        return jnp.zeros((amount,), jnp.int32).at[sequence[jnp.where(places < fixed, places, passed)]].set(jnp.asarray(tallies, jnp.int32))

    tallies = jnp.where(number % 4 == 0, named(packed, number // 4), named(common, number - number // 4 - 1))
    mixed = jax.random.permutation(jax.random.fold_in(own, 3), amount)
    giver, sink = mixed[0:amount // 2 * 2:2], mixed[1:amount // 2 * 2:2]
    margin = jnp.minimum(tallies[giver] - 1, bound - tallies[sink]) // 2
    margin = jnp.where((giver == sequence[0]) | (sink == sequence[0]) | (tallies[sink] == 0), 0, jnp.maximum(margin, 0))
    passed = jax.random.randint(jax.random.fold_in(own, 4), (amount // 2,), 0, 1 << 20) % (margin + 1)
    tallies = tallies.at[giver].add(-passed).at[sink].add(passed)
    labels = jnp.searchsorted(jnp.cumsum(tallies), jnp.arange(rows * top), side="right").astype(jnp.int32)
    grid = labels.reshape(top, rows).T
    grid = grid[jax.random.permutation(jax.random.fold_in(own, 1), rows)]
    turn = jax.random.randint(jax.random.fold_in(own, 2), (rows, 1), 0, top)
    return jnp.take_along_axis(grid, (jnp.arange(top)[None, :] + turn) % top, axis=1)


def portions_of(count, total, bound, slope, full):
    weights = [(1 << 20) // math.isqrt(rank ** slope) + 1 for rank in range(1, count + 1)]
    largest = bound if full else min(bound, max(-(-total // count), total * weights[0] // sum(weights)))
    least = 1 if total - largest >= count - 1 else 0
    holding, surplus = [largest] + [least] * (count - 1), total - largest - least * (count - 1)
    while surplus > 0:
        candidates = [i for i in range(1, count) if holding[i] < largest] or [i for i in range(1, count) if holding[i] < bound]
        pool, remaining = sum([weights[i] for i in candidates]), surplus
        for i in candidates:
            more = min(bound - holding[i], max(1, remaining * weights[i] // pool), surplus)
            holding[i] = holding[i] + more
            surplus = surplus - more
    return np.array(holding)


def gaussian(key, shape, width, most, split=(), kind=jnp.bfloat16):
    array = jax.random.normal(key, shape, jnp.float32) * width
    if len(split) > 0:
        array = levels(key, shape, split, -0.22, 0.18) * array
    return jnp.clip(array, min=-most, max=most).astype(kind)


def setup_inputs(seed: int = 0) -> dict:
    streams_of = jax.random.split(jax.random.key(seed), 16)
    resid = gaussian(streams_of[0], (TOKENS, D), 1.0, 6.0, ((0, 256),))
    conv_b = gaussian(streams_of[1], (TOKENS, CONV), 1.0, 6.0, ((0, 64), (1, 4)))
    conv_c = gaussian(streams_of[2], (TOKENS, CONV), 1.0, 6.0, ((0, 64), (1, 4)))
    conv_x = gaussian(streams_of[3], (TOKENS, CONV), 1.0, 6.0, ((0, 64), (1, 4)))
    conv_taps = gaussian(streams_of[4], (TAPS, CONV), TAPS ** -0.5, 3.5, ((1, 4),))
    out_weight = gaussian(streams_of[5], (CONV, D), CONV ** -0.5, 0.1875, ((0, 4),))
    norm_gain = jnp.clip(1.0 + 0.18 * jax.random.normal(streams_of[6], (D,), jnp.float32), 0.1, 1.9)
    routes_keys = jax.random.split(jax.random.fold_in(streams_of[7], 1), TOKENS // (TOK_DEV // N_TP))
    routes_turns = jax.random.permutation(jax.random.fold_in(streams_of[7], 3), TOKENS // (TOK_DEV // N_TP))
    routes = jax.vmap(lambda own, number: shared_out(jax.random.fold_in(streams_of[7], 2), own, number, TOK_DEV // N_TP, EXPERTS, TOP_K, CAP, 2))(routes_keys, routes_turns).reshape((TOKENS, TOP_K))
    route_weight = jnp.clip(0.2 + 0.8 * jax.random.uniform(streams_of[8], (TOKENS, TOP_K), jnp.float32) ** levels(streams_of[8], (TOKENS, TOP_K), ((0, 64),), -0.2, 0.2), 0.2, 1.0)
    expert_gate = gaussian(streams_of[9], (EXPERTS, D, FF_E), D ** -0.5, 0.125, ((0, 64), (2, 4)))
    expert_up = gaussian(streams_of[10], (EXPERTS, D, FF_E), D ** -0.5, 0.125, ((0, 64), (2, 4)))
    expert_down = gaussian(streams_of[11], (EXPERTS, FF_E, D), FF_E ** -0.5, 0.1875, ((0, 64), (1, 4)))
    shared_gate = gaussian(streams_of[12], (D, FF_E), D ** -0.5, 0.125, ((1, 4),))
    shared_up = gaussian(streams_of[13], (D, FF_E), D ** -0.5, 0.125, ((1, 4),))
    shared_down = gaussian(streams_of[14], (FF_E, D), FF_E ** -0.5, 0.1875, ((0, 4),))
    return {"resid": resid, "conv_b": conv_b, "conv_c": conv_c, "conv_x": conv_x, "conv_taps": conv_taps, "out_weight": out_weight, "norm_gain": norm_gain, "routes": routes, "route_weight": route_weight, "expert_gate": expert_gate, "expert_up": expert_up, "expert_down": expert_down, "shared_gate": shared_gate, "shared_up": shared_up, "shared_down": shared_down}


def round_trip(values):
    return lax.optimization_barrier(values.astype(jnp.bfloat16)).astype(jnp.float32)

def split_down(hidden, down):
    slice_width = down.shape[0] // N_TP
    running = jnp.zeros((hidden.shape[0], down.shape[1]), jnp.float32)
    for column_block in range(N_TP):
        lower = column_block * slice_width
        piece_sum = jnp.dot(hidden[:, lower:lower + slice_width], down[lower:lower + slice_width], preferred_element_type=jnp.float32)
        running = running + round_trip(piece_sum)
    return running

def gated_hidden(block_rows, gate_w, up_w):
    gate_val = jnp.dot(block_rows, gate_w, preferred_element_type=jnp.float32)
    up_val = jnp.dot(block_rows, up_w, preferred_element_type=jnp.float32)
    return (jax.nn.silu(gate_val) * up_val).astype(jnp.bfloat16)

def reference(resid, conv_b, conv_c, conv_x, conv_taps, out_weight, norm_gain, routes, route_weight, expert_gate, expert_up, expert_down, shared_gate, shared_up, shared_down):
    product = conv_c.astype(jnp.float32) * conv_x.astype(jnp.float32)
    padded = jnp.concatenate([jnp.zeros((TAPS - 1, CONV), jnp.float32), product], 0)
    conv_sum = padded[0:TOKENS] * conv_taps[0].astype(jnp.float32)
    for tap_index in range(1, TAPS):
        conv_sum = conv_sum + padded[tap_index:tap_index + TOKENS] * conv_taps[tap_index].astype(jnp.float32)
    mixed_rows = (conv_b.astype(jnp.float32) * conv_sum).astype(jnp.bfloat16)
    projected = split_down(mixed_rows, out_weight)
    middle = (resid.astype(jnp.float32) + projected).astype(jnp.bfloat16)
    middle_float = middle.astype(jnp.float32)
    inv_scale = lax.rsqrt(lax.optimization_barrier(jnp.mean(middle_float * middle_float, axis=-1, keepdims=True)) + 1e-06)
    normed = (middle_float * inv_scale * norm_gain).astype(jnp.bfloat16)
    quarter = TOK_DEV // N_TP
    blocks = TOKENS // quarter
    flat_routes = routes.reshape(blocks, quarter * TOP_K)
    onehot = (flat_routes[:, :, None] == jnp.arange(EXPERTS, dtype=jnp.int32)[None, None, :]).astype(jnp.int32)
    slot_ranks = lax.optimization_barrier(jnp.sum((jnp.cumsum(onehot, axis=1) - 1) * onehot, axis=2))
    per_expert = blocks * CAP
    slot_ids = flat_routes * per_expert + jnp.arange(blocks, dtype=jnp.int32)[:, None] * CAP + slot_ranks
    token_ids = jnp.repeat(jnp.arange(TOKENS, dtype=jnp.int32), TOP_K).reshape(blocks, quarter * TOP_K)
    slot_token = jnp.full((EXPERTS * per_expert,), TOKENS, jnp.int32).at[slot_ids.reshape(-1)].set(token_ids.reshape(-1))
    padded_rows = jnp.concatenate([normed, jnp.zeros((1, D), jnp.bfloat16)], 0)

    def one_expert(expert_index):
        chosen = lax.dynamic_slice_in_dim(slot_token, expert_index * per_expert, per_expert)
        block_rows = padded_rows[chosen]
        hidden = gated_hidden(block_rows, expert_gate[expert_index], expert_up[expert_index])
        return split_down(hidden, expert_down[expert_index]).astype(jnp.bfloat16)
    outputs = lax.map(one_expert, jnp.arange(EXPERTS, dtype=jnp.int32)).reshape(EXPERTS * per_expert, D)
    picked = outputs[slot_ids.reshape(TOKENS, TOP_K)]
    routed = lax.optimization_barrier(jnp.sum(picked.astype(jnp.float32) * route_weight[:, :, None], axis=1))
    shared_hidden = gated_hidden(normed, shared_gate, shared_up)
    shared = split_down(shared_hidden, shared_down)
    return (middle.astype(jnp.float32) + shared + routed).astype(jnp.bfloat16)
```

```python
import functools

import jax
import jax.numpy as jnp
from jax import lax
from jax.experimental import pallas as pl
from jax.experimental.pallas import tpu as pltpu
from jax.sharding import PartitionSpec as P

F32 = jnp.float32
BF16 = jnp.bfloat16
CAP = 4
TP = 4


def remote(src, dst, send_sem, recv_sem, sp, tp):
    return pltpu.make_async_remote_copy(
        src_ref=src,
        dst_ref=dst,
        send_sem=send_sem,
        recv_sem=recv_sem,
        device_id=(sp, tp),
        device_id_type=pl.DeviceIdType.MESH,
    )


def add_into(dst, src):
    dst[...] = (dst[...].astype(F32) + src[...].astype(F32)).astype(BF16)


def kernel(
    groups,
    resid_h, cb_h, cc_h, cx_h, taps, ow_h, gain, routes, rweight,
    wg_h, wu_h, wd_h, sg_h, su_h, sd_h,
    out,
    resid, cb, cc, cx, ow, wg, wu, wd, sg, su, sd,
    prod, mixed, halo, own, proj, proj1, proj2, mid, nrm,
    part, part1, part2,
    disp, wcomb, outgoing, arr, res, res1, res2, summed, ret,
    load_sem, halo_sem, proj_s, proj_r, nrm_s, nrm_r, part_s, part_r,
    a2a_s, a2a_r, ag_s, ag_r, rs_s, rs_r, back_s, back_r,
):
    s = lax.axis_index("sp")
    x = lax.axis_index("tp")
    sp_count = lax.axis_size("sp")
    zs = sp_count // groups
    half = groups // 2
    q, d_model = resid.shape
    dh = d_model // 2
    right = lax.rem(x + 1, TP)
    left = lax.rem(x + TP - 1, TP)
    z = lax.div(s, groups)
    g = lax.rem(s, groups)

    def sp_ahead(dz, dg):
        return lax.rem(z + dz, zs) * groups + lax.rem(g + dg, groups)

    def sp_behind(dz, dg):
        return lax.rem(z + zs - dz, zs) * groups + lax.rem(g + groups - dg, groups)

    def zone(i):
        k = lax.div(i + 1, 2)
        return lax.rem(zs // 2 + zs + (1 - 2 * lax.rem(i, 2)) * k, zs)

    pairs = (
        (cb_h, cb), (cc_h, cc), (cx_h, cx), (ow_h, ow), (resid_h, resid),
        (wg_h.at[0], wg), (wu_h.at[0], wu), (wd_h.at[0], wd), (sg_h, sg), (su_h, su), (sd_h, sd),
    )
    loads = [pltpu.make_async_copy(a, b, load_sem.at[i]) for i, (a, b) in enumerate(pairs)]
    for one in loads:
        one.start()

    barrier = pltpu.get_barrier_semaphore()

    @pl.loop(1, sp_count)
    def _(d):
        pl.semaphore_signal(
            barrier, inc=1, device_id=(lax.rem(s + d, sp_count), x),
            device_id_type=pl.DeviceIdType.MESH,
        )

    for side in (right, left):
        pl.semaphore_signal(
            barrier, inc=1, device_id=(s, side), device_id_type=pl.DeviceIdType.MESH
        )

    slots = sp_count * CAP
    i_slot = lax.broadcasted_iota(jnp.int32, (q, slots), 1)
    rank = lax.rem(i_slot, CAP)
    offset = lax.div(i_slot, CAP)
    e_slot = lax.rem(lax.div(offset, groups) + z, zs) * groups + lax.rem(
        lax.rem(offset, groups) + g, groups
    )
    rows = pl.ds(x * q, q)
    route_0 = routes[rows, 0:1]
    route_1 = routes[rows, 1:2]
    is_0 = e_slot == route_0
    named = jnp.where(is_0 | (e_slot == route_1), 1.0, 0.0)
    before = lax.broadcasted_iota(jnp.int32, (q, q), 0) > lax.broadcasted_iota(
        jnp.int32, (q, q), 1
    )
    count = jnp.dot(
        jnp.where(before, 1.0, 0.0).astype(BF16), named.astype(BF16), preferred_element_type=F32
    )
    held = jnp.where(count == rank.astype(F32), named, 0.0)
    disp[...] = held.T.astype(BF16)
    weight = jnp.where(is_0, rweight[rows, 0:1], rweight[rows, 1:2]) * held
    weight_hi = weight.astype(BF16)
    wcomb[0] = weight_hi
    wcomb[1] = (weight - weight_hi.astype(F32)).astype(BF16)

    for i in range(3):
        loads[i].wait()
    toks = cc.shape[0]
    prod[8 : 8 + toks] = cc[...].astype(F32) * cx[...].astype(F32)
    halo[...] = prod[toks : toks + 8]
    pl.semaphore_wait(barrier, sp_count - 1 + 2)
    halo_copy = remote(
        halo, prod.at[0:8], halo_sem.at[0], halo_sem.at[1], lax.rem(s + 1, sp_count), x
    )
    halo_copy.start()
    loads[3].wait()
    loads[4].wait()
    halo_copy.wait_recv()
    first = jnp.where(s == 0, 0.0, 1.0)
    prod[0:8] = prod[0:8] * first
    conv = prod[6 : 6 + toks] * taps[0:1].astype(F32)
    conv = conv + prod[7 : 7 + toks] * taps[1:2].astype(F32)
    conv = conv + prod[8 : 8 + toks] * taps[2:3].astype(F32)
    mixed[...] = (cb[...].astype(F32) * conv).astype(BF16)

    def ring_sum(b, b1, b2, ssem, rsem):
        def begin():
            remote(b.at[2, 0], b1.at[0], ssem, rsem(0), s, right).start()
            remote(b.at[2, 1], b1.at[1], ssem, rsem(1), s, left).start()
            remote(b.at[3, 1], b2.at[0, 1], ssem, rsem(2), s, right).start()
            remote(b.at[1, 0], b2.at[1, 0], ssem, rsem(3), s, left).start()

        def turn():
            remote(b.at[2, 0], b1.at[0], ssem, rsem(0), s, left).wait_recv()
            add_into(b.at[3, 0], b1.at[0])
            remote(b.at[3, 0], b2.at[0, 0], ssem, rsem(4), s, right).start()
            remote(b.at[2, 1], b1.at[1], ssem, rsem(1), s, right).wait_recv()
            add_into(b.at[1, 1], b1.at[1])
            remote(b.at[1, 1], b2.at[1, 1], ssem, rsem(5), s, left).start()

        def finish():
            remote(b.at[3, 1], b2.at[0, 1], ssem, rsem(2), s, left).wait_recv()
            remote(b.at[1, 0], b2.at[1, 0], ssem, rsem(3), s, right).wait_recv()
            remote(b.at[3, 0], b2.at[0, 0], ssem, rsem(4), s, left).wait_recv()
            remote(b.at[1, 1], b2.at[1, 1], ssem, rsem(5), s, right).wait_recv()

        def drain():
            remote(b.at[0:3], b.at[0:3], ssem, rsem(0), s, right).wait_send()

        return begin, turn, finish, drain

    def ring_gather(b, ssem, rsem):
        def begin():
            remote(b.at[0], b.at[1], ssem, rsem(0), s, right).start()
            remote(b.at[0], b.at[3], ssem, rsem(1), s, left).start()

        def turn():
            remote(b.at[0], b.at[1], ssem, rsem(0), s, left).wait_recv()
            remote(b.at[1, 0], b.at[2, 0], ssem, rsem(2), s, right).start()
            remote(b.at[0], b.at[3], ssem, rsem(1), s, right).wait_recv()
            remote(b.at[3, 1], b.at[2, 1], ssem, rsem(3), s, left).start()

        def finish():
            remote(b.at[1, 0], b.at[2, 0], ssem, rsem(2), s, left).wait_recv()
            remote(b.at[3, 1], b.at[2, 1], ssem, rsem(3), s, right).wait_recv()

        def drain():
            remote(b.at[0:3], b.at[0:3], ssem, rsem(0), s, right).wait_send()

        return begin, turn, finish, drain

    def project(j):
        block = lax.rem(x + TP - j, TP)
        return mixed[pl.ds(pl.multiple_of(block * q, 16), q)]

    proj_begin, proj_turn, proj_finish, proj_drain = ring_sum(
        proj, proj1, proj2, proj_s, lambda k: proj_r.at[k]
    )
    for j in (2, 3, 1):
        for h in range(2):
            proj[j, h] = jnp.dot(
                project(j), ow[:, h * dh : (h + 1) * dh], preferred_element_type=F32
            ).astype(BF16)
    proj_begin()
    for h in range(2):
        own[h] = jnp.dot(project(0), ow[:, h * dh : (h + 1) * dh], preferred_element_type=F32)
    proj_turn()
    proj_finish()
    square = jnp.zeros((q, 1), F32)
    for h in range(2):
        total = own[h] + proj2[0, h].astype(F32) + proj2[1, h].astype(F32)
        m = (resid[:, h * dh : (h + 1) * dh].astype(F32) + total).astype(BF16)
        mid[h] = m
        m = m.astype(F32)
        square = square + jnp.sum(m * m, axis=-1, keepdims=True)
    scale = lax.rsqrt(square * (1.0 / d_model) + 1e-06)
    for h in range(2):
        nrm[0, h] = (mid[h].astype(F32) * scale * gain[:, h * dh : (h + 1) * dh]).astype(BF16)

    nrm_begin, nrm_turn, nrm_finish, nrm_drain = ring_gather(nrm, nrm_s, lambda k: nrm_r.at[k])
    nrm_begin()

    @pl.loop(0, zs)
    def _(i):
        dz = zone(i)
        table = disp[pl.ds(pl.multiple_of(dz * groups * CAP, groups * CAP), groups * CAP)]
        for h in range(2):
            picked = jnp.dot(table, nrm[0, h], preferred_element_type=F32)
            outgoing[dz, :, :, :, h * dh : (h + 1) * dh] = picked.astype(BF16).reshape(
                2, half, CAP, dh
            )
        for dg in range(groups):
            @pl.when((dz != 0) | (dg != 0))
            def _():
                remote(
                    outgoing.at[dz, dg // half, dg % half], arr.at[dz, 0, dg // half, dg % half],
                    a2a_s.at[dz], a2a_r.at[dz], sp_ahead(dz, dg), x,
                ).start()

    arr[0, 0, 0, 0] = outgoing[0, 0, 0]
    for one in loads[5:]:
        one.wait()
    nrm_turn()

    def chain(dz):
        return ring_sum(
            res.at[dz], res1.at[dz], res2.at[dz], rs_s.at[dz], lambda k: rs_r.at[dz, k]
        )

    def spread(dz):
        return ring_gather(arr.at[dz], ag_s.at[dz], lambda k: ag_r.at[dz, k])

    some = ret.at[0 : groups - 1, 0, 0]
    n_rows = TP * groups * CAP
    kc = min(256, d_model)
    nc = min(512, dh)

    def expert(dz):
        gate = jnp.zeros((n_rows, wg.shape[1]), F32)
        up = jnp.zeros((n_rows, wg.shape[1]), F32)
        for k in range(d_model // kc):
            cols = slice(k * kc, (k + 1) * kc)
            block = arr[dz, :, :, :, :, cols].reshape(n_rows, kc)
            gate = gate + jnp.dot(block, wg[cols], preferred_element_type=F32)
            up = up + jnp.dot(block, wu[cols], preferred_element_type=F32)
        hidden = (jax.nn.silu(gate) * up).astype(BF16)
        for n in range(d_model // nc):
            cols = slice(n * nc, (n + 1) * nc)
            res[dz, :, :, :, :, cols] = (
                jnp.dot(hidden, wd[:, cols], preferred_element_type=F32)
                .astype(BF16)
                .reshape(TP, 2, half, CAP, nc)
            )

    part_begin, part_turn, part_finish, part_drain = ring_sum(
        part, part1, part2, part_s, lambda k: part_r.at[k]
    )

    def shared():
        gate = jnp.zeros((TP * q, sg.shape[1]), F32)
        up = jnp.zeros((TP * q, sg.shape[1]), F32)
        for h in range(2):
            block = nrm[:, h].reshape(TP * q, dh)
            gate = gate + jnp.dot(block, sg[h * dh : (h + 1) * dh], preferred_element_type=F32)
            up = up + jnp.dot(block, su[h * dh : (h + 1) * dh], preferred_element_type=F32)
        hidden = (jax.nn.silu(gate) * up).astype(BF16)
        for h in range(2):
            part[:, h] = (
                jnp.dot(hidden, sd[:, h * dh : (h + 1) * dh], preferred_element_type=F32)
                .astype(BF16)
                .reshape(TP, q, dh)
            )

    @pl.loop(0, zs + 4)
    def _(i):
        @pl.when(i < zs)
        def _():
            dz = zone(i)
            wait_zone(arr.at[dz, 0], some, dz, a2a_s, a2a_r, True, s, right)
            spread(dz)[0]()

        @pl.when((i >= 1) & (i < zs + 1))
        def _():
            spread(zone(i - 1))[1]()

        @pl.when(i == 1)
        def _():
            nrm_finish()
            shared()
            part_begin()

        @pl.when((i >= 2) & (i < zs + 2))
        def _():
            dz = zone(i - 2)
            spread(dz)[2]()
            expert(dz)
            chain(dz)[0]()

        @pl.when(i == 2)
        def _():
            part_turn()

        @pl.when((i >= 3) & (i < zs + 3))
        def _():
            chain(zone(i - 3))[1]()

        @pl.when(i >= 4)
        def _():
            dz = zone(i - 4)
            chain(dz)[2]()
            summed[dz] = (
                res[dz, 0].astype(F32) + res2[dz, 0].astype(F32) + res2[dz, 1].astype(F32)
            ).astype(BF16)
            for dg in range(groups):
                @pl.when((dz != 0) | (dg != 0))
                def _():
                    remote(
                        summed.at[dz, dg // half, dg % half], ret.at[dz, dg // half, dg % half],
                        back_s.at[dz], back_r.at[dz], sp_behind(dz, dg), x,
                    ).start()

    ret[0, 0, 0] = summed[0, 0, 0]
    part_finish()

    @pl.loop(0, zs)
    def _(i):
        dz = zone(i)
        wait_zone(ret.at[dz], some, dz, back_s, back_r, True, s, right)

    for n in range(d_model // nc):
        h, c = divmod(n * nc, dh)
        cols = slice(n * nc, (n + 1) * nc)
        local = slice(c, c + nc)
        block = ret[:, :, :, :, cols].reshape(slots, nc)
        total = jnp.dot(wcomb[0], block, preferred_element_type=F32)
        total = total + jnp.dot(wcomb[1], block, preferred_element_type=F32)
        total = total + part[0, h, :, local].astype(F32)
        total = total + part2[0, h, :, local].astype(F32) + part2[1, h, :, local].astype(F32)
        out[:, cols] = (mid[h, :, local].astype(F32) + total).astype(BF16)

    halo_copy.wait_send()
    proj_drain()
    nrm_drain()
    part_drain()

    @pl.loop(0, zs)
    def _(dz):
        wait_zone(outgoing.at[dz], some, dz, a2a_s, a2a_r, False, s, right)
        wait_zone(summed.at[dz], some, dz, back_s, back_r, False, s, right)
        spread(dz)[3]()
        chain(dz)[3]()


def wait_zone(ref, some, dz, ssem, rsem, recv, s, right):
    def fire(a):
        one = remote(a, a, ssem.at[dz], rsem.at[dz], s, right)
        if recv:
            one.wait_recv()
        else:
            one.wait_send()

    @pl.when(dz != 0)
    def _():
        fire(ref)

    @pl.when(dz == 0)
    def _():
        fire(some)


def local(
    resid, conv_b, conv_c, conv_x, conv_taps, out_weight, norm_gain, routes, route_weight,
    expert_gate, expert_up, expert_down, shared_gate, shared_up, shared_down,
):
    sp_count = lax.axis_size("sp")
    groups = max(2, sp_count // 8)
    zs = sp_count // groups
    half = groups // 2
    q, d = resid.shape
    toks, ch = conv_b.shape
    ff = expert_gate.shape[2]
    dh = d // 2
    vmem = pltpu.VMEM
    dma = pltpu.SemaphoreType.DMA
    anywhere = pl.BlockSpec(memory_space=pl.ANY)
    inside = pl.BlockSpec(memory_space=pltpu.VMEM)
    return pl.pallas_call(
        functools.partial(kernel, groups),
        out_shape=jax.ShapeDtypeStruct((q, d), BF16),
        in_specs=[anywhere] * 4 + [inside, anywhere] + [inside] * 3 + [anywhere] * 6,
        out_specs=inside,
        scratch_shapes=[
            vmem((q, d), BF16), vmem((toks, ch), BF16), vmem((toks, ch), BF16),
            vmem((toks, ch), BF16), vmem((ch, d), BF16),
            vmem((d, ff), BF16), vmem((d, ff), BF16), vmem((ff, d), BF16),
            vmem((d, ff), BF16), vmem((d, ff), BF16), vmem((ff, d), BF16),
            vmem((toks + 8, ch), F32), vmem((toks, ch), BF16), vmem((8, ch), F32),
            vmem((2, q, dh), F32),
            vmem((4, 2, q, dh), BF16), vmem((2, q, dh), BF16), vmem((2, 2, q, dh), BF16),
            vmem((2, q, dh), BF16), vmem((4, 2, q, dh), BF16),
            vmem((4, 2, q, dh), BF16), vmem((2, q, dh), BF16), vmem((2, 2, q, dh), BF16),
            vmem((sp_count * CAP, q), BF16), vmem((2, q, sp_count * CAP), BF16),
            vmem((zs, 2, half, CAP, d), BF16),
            vmem((zs, 4, 2, half, CAP, d), BF16),
            vmem((zs, 4, 2, half, CAP, d), BF16),
            vmem((zs, 2, half, CAP, d), BF16),
            vmem((zs, 2, 2, half, CAP, d), BF16),
            vmem((zs, 2, half, CAP, d), BF16),
            vmem((zs, 2, half, CAP, d), BF16),
            dma((11,)), dma((2,)), dma(()), dma((6,)), dma(()), dma((4,)), dma(()), dma((6,)),
            dma((zs,)), dma((zs,)), dma((zs,)), dma((zs, 4)), dma((zs,)), dma((zs, 6)),
            dma((zs,)), dma((zs,)),
        ],
        compiler_params=pltpu.CompilerParams(
            collective_id=0, has_side_effects=True, vmem_limit_bytes=60 * 1024 * 1024
        ),
        name="layer",
    )(
        resid, conv_b, conv_c, conv_x, conv_taps, out_weight, norm_gain.reshape(1, d), routes,
        route_weight, expert_gate, expert_up, expert_down, shared_gate, shared_up, shared_down,
    )


def solution(mesh):
    return jax.shard_map(
        local,
        mesh=mesh,
        in_specs=(
            P(("sp", "tp"), None),
            P("sp", "tp"),
            P("sp", "tp"),
            P("sp", "tp"),
            P(None, "tp"),
            P("tp", None),
            P(),
            P("sp", None),
            P("sp", None),
            P("sp", None, "tp"),
            P("sp", None, "tp"),
            P("sp", "tp", None),
            P(None, "tp"),
            P(None, "tp"),
            P("tp", None),
        ),
        out_specs=P(("sp", "tp"), None),
        check_vma=False,
    )
```

```python
import functools

import jax
import jax.numpy as jnp
from jax import lax
from jax.experimental import pallas as pl
from jax.experimental.pallas import tpu as pltpu
from jax.sharding import PartitionSpec as P

F32 = jnp.float32
BF16 = jnp.bfloat16
CAP = 4
TP = 4
NEAR = 3


def remote(src, dst, send_sem, recv_sem, sp, tp):
    return pltpu.make_async_remote_copy(
        src_ref=src,
        dst_ref=dst,
        send_sem=send_sem,
        recv_sem=recv_sem,
        device_id=(sp, tp),
        device_id_type=pl.DeviceIdType.MESH,
    )


def add_into(dst, src):
    dst[...] = (dst[...].astype(F32) + src[...].astype(F32)).astype(BF16)


def kernel(
    groups,
    resid_h, cb_h, cc_h, cx_h, taps, ow_h, gain, routes, rweight,
    wg_h, wu_h, wd_h, sg_h, su_h, sd_h,
    out,
    resid, cb, cc, cx, ow, wg, wu, wd, sg, su, sd,
    prod, mixed, halo, halo_in, own, proj, proj1, proj2, mid, nrm,
    part, part1, part2, partf,
    rowform, colform, disp, wcomb, outgoing, arr, res, res1, res2, summed, ret,
    near_disp, near_w, near_out, near_arr, near_res, near_ret,
    load_sem, halo_sem, proj_s, proj_r, nrm_s, nrm_r, part_s, part_r,
    a2a_s, a2a_r, ag_s, ag_r, rs_s, rs_r, back_s, back_r, out_s, out_r, home_s, home_r,
):
    s = lax.axis_index("sp")
    x = lax.axis_index("tp")
    sp_count = lax.axis_size("sp")
    zs = sp_count // groups
    far = zs - NEAR
    half = groups // 2
    q, d_model = resid.shape
    dh = d_model // 2
    toks = cc.shape[0]
    msg = TP * CAP
    right = lax.rem(x + 1, TP)
    left = lax.rem(x + TP - 1, TP)
    z = lax.div(s, groups)
    g = lax.rem(s, groups)

    def sp_ahead(dz, dg):
        return lax.rem(z + dz, zs) * groups + lax.rem(g + dg, groups)

    def sp_behind(dz, dg):
        return lax.rem(z + zs - dz, zs) * groups + lax.rem(g + groups - dg, groups)

    def zone(i):
        k = lax.div(i + 1, 2)
        return lax.rem(zs // 2 + zs + (1 - 2 * lax.rem(i, 2)) * k, zs)

    def near_zone(k):
        return jnp.where(k == 0, 1, jnp.where(k == 1, zs - 1, 0))

    pairs = (
        (cc_h, cc), (cx_h, cx), (cb_h, cb), (ow_h, ow), (resid_h, resid),
        (sg_h, sg), (su_h, su), (sd_h, sd), (wg_h.at[0], wg), (wu_h.at[0], wu), (wd_h.at[0], wd),
    )
    loads = [pltpu.make_async_copy(a, b, load_sem.at[i]) for i, (a, b) in enumerate(pairs)]
    for one in loads:
        one.start()

    barrier = pltpu.get_barrier_semaphore()

    for side in (right, left):
        pl.semaphore_signal(
            barrier, inc=1, device_id=(s, side), device_id_type=pl.DeviceIdType.MESH
        )

    @pl.loop(1, sp_count)
    def _(d):
        pl.semaphore_signal(
            barrier, inc=1, device_id=(lax.rem(s + d, sp_count), x),
            device_id_type=pl.DeviceIdType.MESH,
        )

    for i in range(3):
        loads[i].wait()
    prod[0:8] = jnp.zeros((8, prod.shape[1]), F32)
    prod[8 : 8 + toks] = cc[...].astype(F32) * cx[...].astype(F32)
    halo[...] = prod[toks : toks + 8]

    def mix(n):
        conv = prod[6 : 6 + n] * taps[0:1].astype(F32)
        conv = conv + prod[7 : 7 + n] * taps[1:2].astype(F32)
        conv = conv + prod[8 : 8 + n] * taps[2:3].astype(F32)
        mixed[0:n] = (cb[0:n].astype(F32) * conv).astype(BF16)

    def project(j):
        block = lax.rem(x + TP - j, TP)
        return mixed[pl.ds(pl.multiple_of(block * q, 16), q)]

    mix(toks)
    loads[3].wait()
    for j in (2, 3, 1):
        for h in range(2):
            proj[j, h] = jnp.dot(
                project(j), ow[:, h * dh : (h + 1) * dh], preferred_element_type=F32
            ).astype(BF16)

    pl.semaphore_wait(barrier, sp_count - 1 + 2)
    halo_copy = remote(
        halo, halo_in, halo_sem.at[0], halo_sem.at[1], lax.rem(s + 1, sp_count), x
    )
    halo_copy.start()

    def ring_sum(b, b1, b2, ssem, rsem):
        def begin():
            remote(b.at[2, 0], b1.at[0], ssem, rsem(0), s, right).start()
            remote(b.at[2, 1], b1.at[1], ssem, rsem(1), s, left).start()
            remote(b.at[3, 1], b2.at[0, 1], ssem, rsem(2), s, right).start()
            remote(b.at[1, 0], b2.at[1, 0], ssem, rsem(3), s, left).start()

        def turn():
            remote(b.at[2, 0], b1.at[0], ssem, rsem(0), s, left).wait_recv()
            add_into(b.at[3, 0], b1.at[0])
            remote(b.at[3, 0], b2.at[0, 0], ssem, rsem(4), s, right).start()
            remote(b.at[2, 1], b1.at[1], ssem, rsem(1), s, right).wait_recv()
            add_into(b.at[1, 1], b1.at[1])
            remote(b.at[1, 1], b2.at[1, 1], ssem, rsem(5), s, left).start()

        def finish():
            remote(b.at[3, 1], b2.at[0, 1], ssem, rsem(2), s, left).wait_recv()
            remote(b.at[1, 0], b2.at[1, 0], ssem, rsem(3), s, right).wait_recv()
            remote(b.at[3, 0], b2.at[0, 0], ssem, rsem(4), s, left).wait_recv()
            remote(b.at[1, 1], b2.at[1, 1], ssem, rsem(5), s, right).wait_recv()

        def drain():
            remote(b.at[0:3], b.at[0:3], ssem, rsem(0), s, right).wait_send()

        return begin, turn, finish, drain

    def ring_gather(b, ssem, rsem):
        def begin():
            remote(b.at[0], b.at[1], ssem, rsem(0), s, right).start()
            remote(b.at[0], b.at[3], ssem, rsem(1), s, left).start()

        def turn():
            remote(b.at[0], b.at[1], ssem, rsem(0), s, left).wait_recv()
            remote(b.at[1, 0], b.at[2, 0], ssem, rsem(2), s, right).start()
            remote(b.at[0], b.at[3], ssem, rsem(1), s, right).wait_recv()
            remote(b.at[3, 1], b.at[2, 1], ssem, rsem(3), s, left).start()

        def finish():
            remote(b.at[1, 0], b.at[2, 0], ssem, rsem(2), s, left).wait_recv()
            remote(b.at[3, 1], b.at[2, 1], ssem, rsem(3), s, right).wait_recv()

        def drain():
            remote(b.at[0:3], b.at[0:3], ssem, rsem(0), s, right).wait_send()

        return begin, turn, finish, drain

    proj_begin, proj_turn, proj_finish, proj_drain = ring_sum(
        proj, proj1, proj2, proj_s, lambda k: proj_r.at[k]
    )
    halo_copy.wait_recv()
    prod[0:8] = halo_in[...] * jnp.where(s == 0, 0.0, 1.0)
    mix(16)
    for h in range(2):
        proj[x, h, 0:16] = jnp.dot(
            mixed[0:16], ow[:, h * dh : (h + 1) * dh], preferred_element_type=F32
        ).astype(BF16)
    proj_begin()
    for h in range(2):
        own[h] = jnp.dot(project(0), ow[:, h * dh : (h + 1) * dh], preferred_element_type=F32)

    rowform[0:2] = routes[...].astype(F32)
    rowform[2:4] = rweight[...]
    colform[...] = rowform[...].T
    before = lax.broadcasted_iota(jnp.int32, (q, q), 0) > lax.broadcasted_iota(
        jnp.int32, (q, q), 1
    )
    earlier = jnp.where(before, 1.0, 0.0).astype(BF16)

    def table(j, dz, dg, rank, extra):
        expert = lax.rem(dz + z, zs) * groups + lax.rem(dg + g, groups)
        expert = expert.astype(F32)
        rows = pl.ds(pl.multiple_of(lax.rem(x + TP - j, TP) * q, 16), q)
        is_0 = expert == colform[rows, 0:1]
        named = jnp.where(is_0 | (expert == colform[rows, 1:2]), 1.0, 0.0)
        count = jnp.dot(earlier, named.astype(BF16), preferred_element_type=F32)
        held = jnp.where((count == rank.astype(F32)) & extra, named, 0.0)
        weight = jnp.where(is_0, colform[rows, 2:3], colform[rows, 3:4]) * held
        high = weight.astype(BF16)
        return held.T.astype(BF16), high, (weight - high.astype(F32)).astype(BF16)

    far_slots = far * groups * CAP
    i_slot = lax.broadcasted_iota(jnp.int32, (q, far_slots), 1)
    offset = lax.div(i_slot, CAP)
    disp[...], wcomb[0], wcomb[1] = table(
        0, zone(lax.div(offset, groups)), lax.rem(offset, groups), lax.rem(i_slot, CAP),
        i_slot >= 0,
    )

    proj_turn()

    near_slots = NEAR * groups * msg
    n_slot = lax.broadcasted_iota(jnp.int32, (q, near_slots), 1)
    near_offset = lax.div(n_slot, msg)
    for j in range(TP):
        near_disp[j], near_w[0, j], near_w[1, j] = table(
            j, near_zone(lax.div(near_offset, groups)), lax.rem(near_offset, groups),
            lax.rem(n_slot, CAP), lax.rem(lax.div(n_slot, CAP), TP) == j,
        )

    loads[4].wait()
    proj_finish()
    square = jnp.zeros((q, 1), F32)
    for h in range(2):
        total = own[h] + proj2[0, h].astype(F32) + proj2[1, h].astype(F32)
        m = (resid[:, h * dh : (h + 1) * dh].astype(F32) + total).astype(BF16)
        mid[h] = m
        m = m.astype(F32)
        square = square + jnp.sum(m * m, axis=-1, keepdims=True)
    scale = lax.rsqrt(square * (1.0 / d_model) + 1e-06)
    for h in range(2):
        nrm[0, h] = (mid[h].astype(F32) * scale * gain[:, h * dh : (h + 1) * dh]).astype(BF16)

    nrm_begin, nrm_turn, nrm_finish, nrm_drain = ring_gather(nrm, nrm_s, lambda k: nrm_r.at[k])
    nrm_begin()

    zone_rows = groups * CAP

    @pl.loop(0, far)
    def _(i):
        rows = disp[pl.ds(pl.multiple_of(i * zone_rows, zone_rows), zone_rows)]
        for h in range(2):
            picked = jnp.dot(rows, nrm[0, h], preferred_element_type=F32)
            outgoing[i, :, :, :, h * dh : (h + 1) * dh] = picked.astype(BF16).reshape(
                2, half, CAP, dh
            )
        for dg in range(groups):
            remote(
                outgoing.at[i, dg // half, dg % half], arr.at[i, 0, dg // half, dg % half],
                a2a_s.at[i], a2a_r.at[i], sp_ahead(zone(i), dg), x,
            ).start()

    for one in loads[5:]:
        one.wait()
    nrm_turn()
    nrm_finish()

    near_rows = groups * msg

    def near_send(src, dst, k, ssem, rsem, target):
        for dg in range(groups):
            @pl.when((k != NEAR - 1) | (dg != 0))
            def _():
                rows = slice(dg * msg, (dg + 1) * msg)
                remote(
                    src.at[k, rows], dst.at[k, rows], ssem.at[k], rsem.at[k],
                    target(near_zone(k), dg), x,
                ).start()

    def near_wait(ref, k, ssem, rsem, recv):
        def fire(a):
            one = remote(a, a, ssem.at[k], rsem.at[k], s, right)
            if recv:
                one.wait_recv()
            else:
                one.wait_send()

        @pl.when(k != NEAR - 1)
        def _():
            fire(ref.at[k])

        @pl.when(k == NEAR - 1)
        def _():
            fire(ref.at[k, msg:near_rows])

    @pl.loop(0, NEAR)
    def _(k):
        rows = pl.ds(pl.multiple_of(k * near_rows, near_rows), near_rows)
        for h in range(2):
            picked = jnp.dot(near_disp[0, rows], nrm[0, h], preferred_element_type=F32)
            for j in range(1, TP):
                picked = picked + jnp.dot(
                    near_disp[j, rows], nrm[j, h], preferred_element_type=F32
                )
            near_out[k, :, h * dh : (h + 1) * dh] = picked.astype(BF16)
        near_send(near_out, near_arr, k, out_s, out_r, sp_ahead)

    near_arr[NEAR - 1, 0:msg] = near_out[NEAR - 1, 0:msg]

    def chain(i):
        return ring_sum(res.at[i], res1.at[i], res2.at[i], rs_s.at[i], lambda k: rs_r.at[i, k])

    def spread(i):
        return ring_gather(arr.at[i], ag_s.at[i], lambda k: ag_r.at[i, k])

    n_rows = TP * groups * CAP
    kc = min(256, d_model)
    nc = min(512, dh)

    def expert(read, write):
        gate = jnp.zeros((n_rows, wg.shape[1]), F32)
        up = jnp.zeros((n_rows, wg.shape[1]), F32)
        for k in range(d_model // kc):
            cols = slice(k * kc, (k + 1) * kc)
            block = read(cols)
            gate = gate + jnp.dot(block, wg[cols], preferred_element_type=F32)
            up = up + jnp.dot(block, wu[cols], preferred_element_type=F32)
        hidden = (jax.nn.silu(gate) * up).astype(BF16)
        for n in range(d_model // nc):
            cols = slice(n * nc, (n + 1) * nc)
            write(cols, jnp.dot(hidden, wd[:, cols], preferred_element_type=F32).astype(BF16))

    def far_expert(i):
        def write(cols, value):
            res[i, :, :, :, :, cols] = value.reshape(TP, 2, half, CAP, nc)

        expert(lambda cols: arr[i, :, :, :, :, cols].reshape(n_rows, kc), write)

    def near_expert(k):
        def write(cols, value):
            near_res[k, :, cols] = value

        expert(lambda cols: near_arr[k, :, cols], write)

    part_begin, part_turn, part_finish, part_drain = ring_sum(
        part, part1, part2, part_s, lambda k: part_r.at[k]
    )

    def shared():
        gate = jnp.zeros((TP * q, sg.shape[1]), F32)
        up = jnp.zeros((TP * q, sg.shape[1]), F32)
        for h in range(2):
            block = nrm[:, h].reshape(TP * q, dh)
            gate = gate + jnp.dot(block, sg[h * dh : (h + 1) * dh], preferred_element_type=F32)
            up = up + jnp.dot(block, su[h * dh : (h + 1) * dh], preferred_element_type=F32)
        hidden = (jax.nn.silu(gate) * up).astype(BF16)
        for h in range(2):
            partf[:, h] = jnp.dot(
                hidden, sd[:, h * dh : (h + 1) * dh], preferred_element_type=F32
            ).reshape(TP, q, dh)

    def near_combine():
        for j in range(TP):
            for n in range(d_model // nc):
                h, c = divmod(n * nc, dh)
                block = near_ret[:, :, n * nc : (n + 1) * nc].reshape(near_slots, nc)
                total = partf[j, h, :, c : c + nc]
                total = total + jnp.dot(near_w[0, j], block, preferred_element_type=F32)
                total = total + jnp.dot(near_w[1, j], block, preferred_element_type=F32)
                part[j, h, :, c : c + nc] = total.astype(BF16)

    @pl.loop(0, STEPS(far))
    def _(i):
        @pl.when(i < far)
        def _():
            a = arr.at[i, 0]
            remote(a, a, a2a_s.at[i], a2a_r.at[i], s, right).wait_recv()
            spread(i)[0]()

        @pl.when((i >= 1) & (i < far + 1))
        def _():
            spread(i - 1)[1]()

        @pl.when(i == 1)
        def _():
            shared()

        @pl.when((i >= 2) & (i < far + 2))
        def _():
            spread(i - 2)[2]()
            far_expert(i - 2)
            chain(i - 2)[0]()

        @pl.when((i >= 2) & (i < 2 + NEAR))
        def _():
            k = i - 2
            near_wait(near_arr, k, out_s, out_r, True)
            near_expert(k)
            near_send(near_res, near_ret, k, home_s, home_r, sp_behind)

        @pl.when((i >= 3) & (i < far + 3))
        def _():
            chain(i - 3)[1]()

        @pl.when((i >= 4) & (i < far + 4))
        def _():
            k = i - 4
            chain(k)[2]()
            summed[k] = (
                res[k, 0].astype(F32) + res2[k, 0].astype(F32) + res2[k, 1].astype(F32)
            ).astype(BF16)
            for dg in range(groups):
                remote(
                    summed.at[k, dg // half, dg % half], ret.at[k, dg // half, dg % half],
                    back_s.at[k], back_r.at[k], sp_behind(zone(k), dg), x,
                ).start()

        @pl.when(i == NEAR + 3)
        def _():
            near_ret[NEAR - 1, 0:msg] = near_res[NEAR - 1, 0:msg]
            for k in range(NEAR):
                near_wait(near_ret, k, home_s, home_r, True)
            near_combine()
            part_begin()

        @pl.when(i == NEAR + 4)
        def _():
            part_turn()

    part_finish()

    @pl.loop(0, far)
    def _(i):
        a = ret.at[i]
        remote(a, a, back_s.at[i], back_r.at[i], s, right).wait_recv()

    for n in range(d_model // nc):
        h, c = divmod(n * nc, dh)
        cols = slice(n * nc, (n + 1) * nc)
        local = slice(c, c + nc)
        block = ret[:, :, :, :, cols].reshape(far_slots, nc)
        total = jnp.dot(wcomb[0], block, preferred_element_type=F32)
        total = total + jnp.dot(wcomb[1], block, preferred_element_type=F32)
        total = total + part[0, h, :, local].astype(F32)
        total = total + part2[0, h, :, local].astype(F32) + part2[1, h, :, local].astype(F32)
        out[:, cols] = (mid[h, :, local].astype(F32) + total).astype(BF16)

    halo_copy.wait_send()
    proj_drain()
    nrm_drain()
    part_drain()

    @pl.loop(0, far)
    def _(i):
        a = outgoing.at[i]
        remote(a, a, a2a_s.at[i], a2a_r.at[i], s, right).wait_send()
        b = summed.at[i]
        remote(b, b, back_s.at[i], back_r.at[i], s, right).wait_send()
        spread(i)[3]()
        chain(i)[3]()

    for k in range(NEAR):
        near_wait(near_out, k, out_s, out_r, False)
        near_wait(near_res, k, home_s, home_r, False)


def STEPS(far):
    return max(far + 4, NEAR + 5)


def local(
    resid, conv_b, conv_c, conv_x, conv_taps, out_weight, norm_gain, routes, route_weight,
    expert_gate, expert_up, expert_down, shared_gate, shared_up, shared_down,
):
    sp_count = lax.axis_size("sp")
    groups = max(2, sp_count // 8)
    zs = sp_count // groups
    half = groups // 2
    far = zs - NEAR
    near_slots = NEAR * groups * TP * CAP
    q, d = resid.shape
    toks, ch = conv_b.shape
    ff = expert_gate.shape[2]
    dh = d // 2
    vmem = pltpu.VMEM
    dma = pltpu.SemaphoreType.DMA
    anywhere = pl.BlockSpec(memory_space=pl.ANY)
    inside = pl.BlockSpec(memory_space=pltpu.VMEM)
    return pl.pallas_call(
        functools.partial(kernel, groups),
        out_shape=jax.ShapeDtypeStruct((q, d), BF16),
        in_specs=[anywhere] * 4 + [inside, anywhere] + [inside] * 3 + [anywhere] * 6,
        out_specs=inside,
        scratch_shapes=[
            vmem((q, d), BF16), vmem((toks, ch), BF16), vmem((toks, ch), BF16),
            vmem((toks, ch), BF16), vmem((ch, d), BF16),
            vmem((d, ff), BF16), vmem((d, ff), BF16), vmem((ff, d), BF16),
            vmem((d, ff), BF16), vmem((d, ff), BF16), vmem((ff, d), BF16),
            vmem((toks + 8, ch), F32), vmem((toks, ch), BF16), vmem((8, ch), F32), vmem((8, ch), F32),
            vmem((2, q, dh), F32),
            vmem((4, 2, q, dh), BF16), vmem((2, q, dh), BF16), vmem((2, 2, q, dh), BF16),
            vmem((2, q, dh), BF16), vmem((4, 2, q, dh), BF16),
            vmem((4, 2, q, dh), BF16), vmem((2, q, dh), BF16), vmem((2, 2, q, dh), BF16),
            vmem((4, 2, q, dh), F32),
            vmem((8, toks), F32), vmem((toks, 8), F32),
            vmem((far * groups * CAP, q), BF16), vmem((2, q, far * groups * CAP), BF16),
            vmem((far, 2, half, CAP, d), BF16),
            vmem((far, 4, 2, half, CAP, d), BF16),
            vmem((far, 4, 2, half, CAP, d), BF16),
            vmem((far, 2, half, CAP, d), BF16),
            vmem((far, 2, 2, half, CAP, d), BF16),
            vmem((far, 2, half, CAP, d), BF16),
            vmem((far, 2, half, CAP, d), BF16),
            vmem((TP, near_slots, q), BF16), vmem((2, TP, q, near_slots), BF16),
            vmem((NEAR, groups * TP * CAP, d), BF16), vmem((NEAR, groups * TP * CAP, d), BF16),
            vmem((NEAR, groups * TP * CAP, d), BF16), vmem((NEAR, groups * TP * CAP, d), BF16),
            dma((11,)), dma((2,)), dma(()), dma((6,)), dma(()), dma((4,)), dma(()), dma((6,)),
            dma((far,)), dma((far,)), dma((far,)), dma((far, 4)), dma((far,)), dma((far, 6)),
            dma((far,)), dma((far,)), dma((NEAR,)), dma((NEAR,)), dma((NEAR,)), dma((NEAR,)),
        ],
        compiler_params=pltpu.CompilerParams(
            collective_id=0, has_side_effects=True, vmem_limit_bytes=60 * 1024 * 1024
        ),
        name="layer",
    )(
        resid, conv_b, conv_c, conv_x, conv_taps, out_weight, norm_gain.reshape(1, d), routes.T,
        route_weight.T, expert_gate, expert_up, expert_down, shared_gate, shared_up, shared_down,
    )


def solution(mesh):
    return jax.shard_map(
        local,
        mesh=mesh,
        in_specs=(
            P(("sp", "tp"), None),
            P("sp", "tp"),
            P("sp", "tp"),
            P("sp", "tp"),
            P(None, "tp"),
            P("tp", None),
            P(),
            P("sp", None),
            P("sp", None),
            P("sp", None, "tp"),
            P("sp", None, "tp"),
            P("sp", "tp", None),
            P(None, "tp"),
            P(None, "tp"),
            P("tp", None),
        ),
        out_specs=P(("sp", "tp"), None),
        check_vma=False,
    )
```

```python
import functools

import jax
import jax.numpy as jnp
from jax import lax
from jax.experimental import pallas as pl
from jax.experimental.pallas import tpu as pltpu
from jax.sharding import PartitionSpec as P

F32 = jnp.float32
BF16 = jnp.bfloat16
CAP = 4
TP = 4
NEAR = 3
NEAR_STEP = 4


def remote(src, dst, send_sem, recv_sem, sp, tp):
    return pltpu.make_async_remote_copy(
        src_ref=src,
        dst_ref=dst,
        send_sem=send_sem,
        recv_sem=recv_sem,
        device_id=(sp, tp),
        device_id_type=pl.DeviceIdType.MESH,
    )


def add_into(dst, src):
    dst[...] = (dst[...].astype(F32) + src[...].astype(F32)).astype(BF16)


def kernel(
    groups,
    resid_h, cb_h, cc_h, cx_h, taps, ow_h, gain, routes, rweight,
    wg_h, wu_h, wd_h, sg_h, su_h, sd_h,
    out,
    resid, cb, cc, cx, ow, wg, wu, wd, sg, su, sd,
    prod, mixed, halo, halo_in, own, proj, proj1, proj2, mid, nrm,
    part, part1, part2, partf,
    rowform, colform, disp, wcomb, outgoing, arr, res, res1, res2, summed, ret,
    near_disp, near_w, near_out, near_arr, near_res, near_ret,
    load_sem, halo_sem, proj_s, proj_r, nrm_s, nrm_r, part_s, part_r,
    a2a_s, a2a_r, ag_s, ag_r, rs_s, rs_r, back_s, back_r, out_s, out_r, home_s, home_r, known,
):
    s = lax.axis_index("sp")
    x = lax.axis_index("tp")
    sp_count = lax.axis_size("sp")
    zs = sp_count // groups
    far = zs - NEAR
    half = groups // 2
    q, d_model = resid.shape
    dh = d_model // 2
    toks = cc.shape[0]
    msg = TP * CAP
    right = lax.rem(x + 1, TP)
    left = lax.rem(x + TP - 1, TP)
    z = lax.div(s, groups)
    g = lax.rem(s, groups)

    def sp_ahead(dz, dg):
        return lax.rem(z + dz, zs) * groups + lax.rem(g + dg, groups)

    def sp_behind(dz, dg):
        return lax.rem(z + zs - dz, zs) * groups + lax.rem(g + groups - dg, groups)

    order = sorted(range(2, zs - 1), key=lambda dz: (min(dz, zs - dz) == 2, min(dz, zs - dz)))

    def zone(i):
        dz = order[0]
        for n, other in enumerate(order[1:]):
            dz = jnp.where(i == n + 1, other, dz)
        return dz

    def near_zone(k):
        return jnp.where(k == 0, 1, jnp.where(k == 1, zs - 1, 0))

    pairs = (
        (cc_h, cc), (cx_h, cx), (cb_h, cb), (ow_h, ow), (resid_h, resid),
        (sg_h, sg), (su_h, su), (sd_h, sd), (wg_h.at[0], wg), (wu_h.at[0], wu), (wd_h.at[0], wd),
    )
    loads = [pltpu.make_async_copy(a, b, load_sem.at[i]) for i, (a, b) in enumerate(pairs)]
    for one in loads:
        one.start()

    barrier = pltpu.get_barrier_semaphore()

    def tell(sem, sp, tp):
        pl.semaphore_signal(
            sem, inc=1, device_id=(sp, tp), device_id_type=pl.DeviceIdType.MESH
        )

    core = z * groups + g + 1 - 2 * lax.rem(g, 2)
    y_sides = (sp_ahead(0, 2), sp_behind(0, 2)) if groups > 2 else ()
    z_sides = (sp_ahead(1, 0), sp_behind(1, 0))
    ring_sides = (lax.rem(s + 1, sp_count), lax.rem(s + sp_count - 1, sp_count))
    for side in (right, left):
        tell(barrier, s, side)
    for side in ring_sides + (core,) + y_sides + z_sides:
        tell(barrier, side, x)
    n_near = 2 + 3 + len(y_sides) + 2
    rounds = [(core,)] + [y_sides] * (groups // 4) + [z_sides] * (zs // 2)

    def pass_on(k):
        if k < len(rounds):
            for side in rounds[k]:
                tell(known.at[k], side, x)

    def learn(k):
        if k < len(rounds):
            pl.semaphore_wait(known.at[k], len(rounds[k]))

    for i in range(3):
        loads[i].wait()
    prod[0:8] = jnp.zeros((8, prod.shape[1]), F32)
    prod[8 : 8 + toks] = cc[...].astype(F32) * cx[...].astype(F32)
    halo[...] = prod[toks : toks + 8]

    def mix(n):
        conv = prod[6 : 6 + n] * taps[0:1].astype(F32)
        conv = conv + prod[7 : 7 + n] * taps[1:2].astype(F32)
        conv = conv + prod[8 : 8 + n] * taps[2:3].astype(F32)
        mixed[0:n] = (cb[0:n].astype(F32) * conv).astype(BF16)

    def project(j):
        block = lax.rem(x + TP - j, TP)
        return mixed[pl.ds(pl.multiple_of(block * q, 16), q)]

    mix(toks)
    loads[3].wait()
    for j in (2, 3, 1):
        for h in range(2):
            proj[j, h] = jnp.dot(
                project(j), ow[:, h * dh : (h + 1) * dh], preferred_element_type=F32
            ).astype(BF16)

    pl.semaphore_wait(barrier, n_near)
    pass_on(0)
    halo_copy = remote(
        halo, halo_in, halo_sem.at[0], halo_sem.at[1], lax.rem(s + 1, sp_count), x
    )
    halo_copy.start()

    def ring_sum(b, b1, b2, ssem, rsem):
        def begin():
            remote(b.at[2, 0], b1.at[0], ssem, rsem(0), s, right).start()
            remote(b.at[2, 1], b1.at[1], ssem, rsem(1), s, left).start()
            remote(b.at[3, 1], b2.at[0, 1], ssem, rsem(2), s, right).start()
            remote(b.at[1, 0], b2.at[1, 0], ssem, rsem(3), s, left).start()

        def turn():
            remote(b.at[2, 0], b1.at[0], ssem, rsem(0), s, left).wait_recv()
            add_into(b.at[3, 0], b1.at[0])
            remote(b.at[3, 0], b2.at[0, 0], ssem, rsem(4), s, right).start()
            remote(b.at[2, 1], b1.at[1], ssem, rsem(1), s, right).wait_recv()
            add_into(b.at[1, 1], b1.at[1])
            remote(b.at[1, 1], b2.at[1, 1], ssem, rsem(5), s, left).start()

        def finish():
            remote(b.at[3, 1], b2.at[0, 1], ssem, rsem(2), s, left).wait_recv()
            remote(b.at[1, 0], b2.at[1, 0], ssem, rsem(3), s, right).wait_recv()
            remote(b.at[3, 0], b2.at[0, 0], ssem, rsem(4), s, left).wait_recv()
            remote(b.at[1, 1], b2.at[1, 1], ssem, rsem(5), s, right).wait_recv()

        def drain():
            remote(b.at[0:3], b.at[0:3], ssem, rsem(0), s, right).wait_send()

        return begin, turn, finish, drain

    def ring_gather(b, ssem, rsem):
        def begin():
            remote(b.at[0], b.at[1], ssem, rsem(0), s, right).start()
            remote(b.at[0], b.at[3], ssem, rsem(1), s, left).start()

        def turn():
            remote(b.at[0], b.at[1], ssem, rsem(0), s, left).wait_recv()
            remote(b.at[1, 0], b.at[2, 0], ssem, rsem(2), s, right).start()
            remote(b.at[0], b.at[3], ssem, rsem(1), s, right).wait_recv()
            remote(b.at[3, 1], b.at[2, 1], ssem, rsem(3), s, left).start()

        def finish():
            remote(b.at[1, 0], b.at[2, 0], ssem, rsem(2), s, left).wait_recv()
            remote(b.at[3, 1], b.at[2, 1], ssem, rsem(3), s, right).wait_recv()

        def drain():
            remote(b.at[0:3], b.at[0:3], ssem, rsem(0), s, right).wait_send()

        return begin, turn, finish, drain

    proj_begin, proj_turn, proj_finish, proj_drain = ring_sum(
        proj, proj1, proj2, proj_s, lambda k: proj_r.at[k]
    )
    learn(0)
    pass_on(1)
    halo_copy.wait_recv()
    prod[0:8] = halo_in[...] * jnp.where(s == 0, 0.0, 1.0)
    mix(16)
    for h in range(2):
        proj[x, h, 0:16] = jnp.dot(
            mixed[0:16], ow[:, h * dh : (h + 1) * dh], preferred_element_type=F32
        ).astype(BF16)
    proj_begin()
    learn(1)
    pass_on(2)
    for h in range(2):
        own[h] = jnp.dot(project(0), ow[:, h * dh : (h + 1) * dh], preferred_element_type=F32)

    learn(2)
    pass_on(3)

    rowform[0:2] = routes[...].astype(F32)
    rowform[2:4] = rweight[...]
    colform[...] = rowform[...].T
    before = lax.broadcasted_iota(jnp.int32, (q, q), 0) > lax.broadcasted_iota(
        jnp.int32, (q, q), 1
    )
    earlier = jnp.where(before, 1.0, 0.0).astype(BF16)

    def table(j, dz, dg, rank, extra):
        expert = lax.rem(dz + z, zs) * groups + lax.rem(dg + g, groups)
        expert = expert.astype(F32)
        rows = pl.ds(pl.multiple_of(lax.rem(x + TP - j, TP) * q, 16), q)
        is_0 = expert == colform[rows, 0:1]
        named = jnp.where(is_0 | (expert == colform[rows, 1:2]), 1.0, 0.0)
        count = jnp.dot(earlier, named.astype(BF16), preferred_element_type=F32)
        held = jnp.where((count == rank.astype(F32)) & extra, named, 0.0)
        weight = jnp.where(is_0, colform[rows, 2:3], colform[rows, 3:4]) * held
        high = weight.astype(BF16)
        return held.T.astype(BF16), high, (weight - high.astype(F32)).astype(BF16)

    far_slots = far * groups * CAP
    i_slot = lax.broadcasted_iota(jnp.int32, (q, far_slots), 1)
    offset = lax.div(i_slot, CAP)
    disp[...], wcomb[0:q], wcomb[q : 2 * q] = table(
        0, zone(lax.div(offset, groups)), lax.rem(offset, groups), lax.rem(i_slot, CAP),
        i_slot >= 0,
    )

    learn(3)
    pass_on(4)
    proj_turn()

    near_slots = NEAR * groups * msg
    n_slot = lax.broadcasted_iota(jnp.int32, (q, near_slots), 1)
    near_offset = lax.div(n_slot, msg)
    for j in range(TP):
        high, low = pl.ds(j * q, q), pl.ds((TP + j) * q, q)
        near_disp[j], near_w[high], near_w[low] = table(
            j, near_zone(lax.div(near_offset, groups)), lax.rem(near_offset, groups),
            lax.rem(n_slot, CAP), lax.rem(lax.div(n_slot, CAP), TP) == j,
        )
        learn(4 + j)
        pass_on(5 + j)

    loads[4].wait()
    proj_finish()
    square = jnp.zeros((q, 1), F32)
    for h in range(2):
        total = own[h] + proj2[0, h].astype(F32) + proj2[1, h].astype(F32)
        m = (resid[:, h * dh : (h + 1) * dh].astype(F32) + total).astype(BF16)
        mid[h] = m
        m = m.astype(F32)
        square = square + jnp.sum(m * m, axis=-1, keepdims=True)
    scale = lax.rsqrt(square * (1.0 / d_model) + 1e-06)
    for h in range(2):
        nrm[0, h] = (mid[h].astype(F32) * scale * gain[:, h * dh : (h + 1) * dh]).astype(BF16)

    nrm_begin, nrm_turn, nrm_finish, nrm_drain = ring_gather(nrm, nrm_s, lambda k: nrm_r.at[k])
    nrm_begin()

    zone_rows = groups * CAP

    def far_dispatch(low, high):
        @pl.loop(low, high)
        def _(i):
            rows = disp[pl.ds(pl.multiple_of(i * zone_rows, zone_rows), zone_rows)]
            for h in range(2):
                picked = jnp.dot(rows, nrm[0, h], preferred_element_type=F32)
                outgoing[i, :, :, :, h * dh : (h + 1) * dh] = picked.astype(BF16).reshape(
                    2, half, CAP, dh
                )
            for dg in range(groups):
                remote(
                    outgoing.at[i, dg // half, dg % half], arr.at[i, 0, dg // half, dg % half],
                    a2a_s.at[i], a2a_r.at[i], sp_ahead(zone(i), dg), x,
                ).start()

    urgent = min(3, far)
    far_dispatch(0, urgent)
    for one in loads[5:]:
        one.wait()
    nrm_turn()
    far_dispatch(urgent, far)

    near_rows = groups * msg

    def near_send(src, dst, k, ssem, rsem, target):
        for dg in range(groups):
            @pl.when((k != NEAR - 1) | (dg != 0))
            def _():
                rows = slice(dg * msg, (dg + 1) * msg)
                remote(
                    src.at[k, rows], dst.at[k, rows], ssem.at[k], rsem.at[k],
                    target(near_zone(k), dg), x,
                ).start()

    def near_wait(ref, k, ssem, rsem, recv):
        def fire(a):
            one = remote(a, a, ssem.at[k], rsem.at[k], s, right)
            if recv:
                one.wait_recv()
            else:
                one.wait_send()

        @pl.when(k != NEAR - 1)
        def _():
            fire(ref.at[k])

        @pl.when(k == NEAR - 1)
        def _():
            fire(ref.at[k, msg:near_rows])

    def near_dispatch():
        @pl.loop(0, NEAR)
        def _(k):
            rows = pl.ds(pl.multiple_of(k * near_rows, near_rows), near_rows)
            for h in range(2):
                picked = jnp.dot(near_disp[0, rows], nrm[0, h], preferred_element_type=F32)
                for j in range(1, TP):
                    picked = picked + jnp.dot(
                        near_disp[j, rows], nrm[j, h], preferred_element_type=F32
                    )
                near_out[k, :, h * dh : (h + 1) * dh] = picked.astype(BF16)
            near_send(near_out, near_arr, k, out_s, out_r, sp_ahead)

        near_arr[NEAR - 1, 0:msg] = near_out[NEAR - 1, 0:msg]

    def chain(i):
        return ring_sum(res.at[i], res1.at[i], res2.at[i], rs_s.at[i], lambda k: rs_r.at[i, k])

    def spread(i):
        return ring_gather(arr.at[i], ag_s.at[i], lambda k: ag_r.at[i, k])

    n_rows = TP * groups * CAP
    kc = min(256, d_model)
    nc = min(512, dh)

    def expert(read, write):
        gate = jnp.zeros((n_rows, wg.shape[1]), F32)
        up = jnp.zeros((n_rows, wg.shape[1]), F32)
        for k in range(d_model // kc):
            cols = slice(k * kc, (k + 1) * kc)
            block = read(cols)
            gate = gate + jnp.dot(block, wg[cols], preferred_element_type=F32)
            up = up + jnp.dot(block, wu[cols], preferred_element_type=F32)
        hidden = (jax.nn.silu(gate) * up).astype(BF16)
        for n in range(d_model // nc):
            cols = slice(n * nc, (n + 1) * nc)
            write(cols, jnp.dot(hidden, wd[:, cols], preferred_element_type=F32).astype(BF16))

    def far_expert(i):
        def write(cols, value):
            res[i, :, :, :, :, cols] = value.reshape(TP, 2, half, CAP, nc)

        expert(lambda cols: arr[i, :, :, :, :, cols].reshape(n_rows, kc), write)

    def near_expert(k):
        def write(cols, value):
            near_res[k, :, cols] = value

        expert(lambda cols: near_arr[k, :, cols], write)

    part_begin, part_turn, part_finish, part_drain = ring_sum(
        part, part1, part2, part_s, lambda k: part_r.at[k]
    )

    def shared():
        gate = jnp.zeros((TP * q, sg.shape[1]), F32)
        up = jnp.zeros((TP * q, sg.shape[1]), F32)
        for h in range(2):
            block = nrm[:, h].reshape(TP * q, dh)
            gate = gate + jnp.dot(block, sg[h * dh : (h + 1) * dh], preferred_element_type=F32)
            up = up + jnp.dot(block, su[h * dh : (h + 1) * dh], preferred_element_type=F32)
        hidden = (jax.nn.silu(gate) * up).astype(BF16)
        for h in range(2):
            partf[:, h] = jnp.dot(
                hidden, sd[:, h * dh : (h + 1) * dh], preferred_element_type=F32
            ).reshape(TP, q, dh)

    def near_combine():
        for n in range(d_model // kc):
            h, c = divmod(n * kc, dh)
            block = near_ret[:, :, n * kc : (n + 1) * kc].reshape(near_slots, kc)
            both = jnp.dot(near_w[...], block, preferred_element_type=F32)
            total = partf[:, h, :, c : c + kc] + (both[: TP * q] + both[TP * q :]).reshape(
                TP, q, kc
            )
            part[:, h, :, c : c + kc] = total.astype(BF16)

    def far_combine():
        for n in range(d_model // nc):
            h, c = divmod(n * nc, dh)
            block = ret[:, :, :, :, n * nc : (n + 1) * nc].reshape(far_slots, nc)
            both = jnp.dot(wcomb[...], block, preferred_element_type=F32)
            own[h, :, c : c + nc] = (
                both[:q] + both[q:] + mid[h, :, c : c + nc].astype(F32)
                + part[0, h, :, c : c + nc].astype(F32)
            )

    @pl.loop(0, far + 4)
    def _(i):
        @pl.when(i < far)
        def _():
            a = arr.at[i, 0]
            remote(a, a, a2a_s.at[i], a2a_r.at[i], s, right).wait_recv()
            spread(i)[0]()

        @pl.when(i == 0)
        def _():
            nrm_finish()
            near_dispatch()

        @pl.when((i >= 1) & (i < far + 1))
        def _():
            spread(i - 1)[1]()

        @pl.when(i == 1)
        def _():
            shared()

        @pl.when((i >= 2) & (i < far + 2))
        def _():
            spread(i - 2)[2]()
            far_expert(i - 2)
            chain(i - 2)[0]()

        @pl.when(i == NEAR_STEP)
        def _():
            @pl.loop(0, NEAR)
            def _(k):
                near_wait(near_arr, k, out_s, out_r, True)
                near_expert(k)
                near_send(near_res, near_ret, k, home_s, home_r, sp_behind)

        @pl.when((i >= 3) & (i < far + 3))
        def _():
            chain(i - 3)[1]()

        @pl.when((i >= 4) & (i < far + 4))
        def _():
            k = i - 4
            chain(k)[2]()
            summed[k] = (
                res[k, 0].astype(F32) + res2[k, 0].astype(F32) + res2[k, 1].astype(F32)
            ).astype(BF16)
            for dg in range(groups):
                remote(
                    summed.at[k, dg // half, dg % half], ret.at[k, dg // half, dg % half],
                    back_s.at[k], back_r.at[k], sp_behind(zone(k), dg), x,
                ).start()

    near_ret[NEAR - 1, 0:msg] = near_res[NEAR - 1, 0:msg]
    for k in range(NEAR):
        near_wait(near_ret, k, home_s, home_r, True)
    near_combine()
    part_begin()
    part_turn()

    @pl.loop(0, far)
    def _(i):
        a = ret.at[i]
        remote(a, a, back_s.at[i], back_r.at[i], s, right).wait_recv()

    far_combine()
    part_finish()
    for h in range(2):
        total = own[h] + part2[0, h].astype(F32) + part2[1, h].astype(F32)
        out[:, h * dh : (h + 1) * dh] = total.astype(BF16)

    halo_copy.wait_send()
    proj_drain()
    nrm_drain()
    part_drain()

    @pl.loop(0, far)
    def _(i):
        a = outgoing.at[i]
        remote(a, a, a2a_s.at[i], a2a_r.at[i], s, right).wait_send()
        b = summed.at[i]
        remote(b, b, back_s.at[i], back_r.at[i], s, right).wait_send()
        spread(i)[3]()
        chain(i)[3]()

    for k in range(NEAR):
        near_wait(near_out, k, out_s, out_r, False)
        near_wait(near_res, k, home_s, home_r, False)


def local(
    resid, conv_b, conv_c, conv_x, conv_taps, out_weight, norm_gain, routes, route_weight,
    expert_gate, expert_up, expert_down, shared_gate, shared_up, shared_down,
):
    sp_count = lax.axis_size("sp")
    groups = max(2, sp_count // 8)
    zs = sp_count // groups
    half = groups // 2
    far = zs - NEAR
    near_slots = NEAR * groups * TP * CAP
    q, d = resid.shape
    toks, ch = conv_b.shape
    ff = expert_gate.shape[2]
    dh = d // 2
    vmem = pltpu.VMEM
    dma = pltpu.SemaphoreType.DMA
    anywhere = pl.BlockSpec(memory_space=pl.ANY)
    inside = pl.BlockSpec(memory_space=pltpu.VMEM)
    return pl.pallas_call(
        functools.partial(kernel, groups),
        out_shape=jax.ShapeDtypeStruct((q, d), BF16),
        in_specs=[anywhere] * 4 + [inside, anywhere] + [inside] * 3 + [anywhere] * 6,
        out_specs=inside,
        scratch_shapes=[
            vmem((q, d), BF16), vmem((toks, ch), BF16), vmem((toks, ch), BF16),
            vmem((toks, ch), BF16), vmem((ch, d), BF16),
            vmem((d, ff), BF16), vmem((d, ff), BF16), vmem((ff, d), BF16),
            vmem((d, ff), BF16), vmem((d, ff), BF16), vmem((ff, d), BF16),
            vmem((toks + 8, ch), F32), vmem((toks, ch), BF16), vmem((8, ch), F32), vmem((8, ch), F32),
            vmem((2, q, dh), F32),
            vmem((4, 2, q, dh), BF16), vmem((2, q, dh), BF16), vmem((2, 2, q, dh), BF16),
            vmem((2, q, dh), BF16), vmem((4, 2, q, dh), BF16),
            vmem((4, 2, q, dh), BF16), vmem((2, q, dh), BF16), vmem((2, 2, q, dh), BF16),
            vmem((4, 2, q, dh), F32),
            vmem((8, toks), F32), vmem((toks, 8), F32),
            vmem((far * groups * CAP, q), BF16), vmem((2 * q, far * groups * CAP), BF16),
            vmem((far, 2, half, CAP, d), BF16),
            vmem((far, 4, 2, half, CAP, d), BF16),
            vmem((far, 4, 2, half, CAP, d), BF16),
            vmem((far, 2, half, CAP, d), BF16),
            vmem((far, 2, 2, half, CAP, d), BF16),
            vmem((far, 2, half, CAP, d), BF16),
            vmem((far, 2, half, CAP, d), BF16),
            vmem((TP, near_slots, q), BF16), vmem((2 * TP * q, near_slots), BF16),
            vmem((NEAR, groups * TP * CAP, d), BF16), vmem((NEAR, groups * TP * CAP, d), BF16),
            vmem((NEAR, groups * TP * CAP, d), BF16), vmem((NEAR, groups * TP * CAP, d), BF16),
            dma((11,)), dma((2,)), dma(()), dma((6,)), dma(()), dma((4,)), dma(()), dma((6,)),
            dma((far,)), dma((far,)), dma((far,)), dma((far, 4)), dma((far,)), dma((far, 6)),
            dma((far,)), dma((far,)), dma((NEAR,)), dma((NEAR,)), dma((NEAR,)), dma((NEAR,)),
            pltpu.SemaphoreType.REGULAR((8,)),
        ],
        compiler_params=pltpu.CompilerParams(
            collective_id=0, has_side_effects=True, vmem_limit_bytes=60 * 1024 * 1024
        ),
        name="layer",
    )(
        resid, conv_b, conv_c, conv_x, conv_taps, out_weight, norm_gain.reshape(1, d), routes.T,
        route_weight.T, expert_gate, expert_up, expert_down, shared_gate, shared_up, shared_down,
    )


def solution(mesh):
    return jax.shard_map(
        local,
        mesh=mesh,
        in_specs=(
            P(("sp", "tp"), None),
            P("sp", "tp"),
            P("sp", "tp"),
            P("sp", "tp"),
            P(None, "tp"),
            P("tp", None),
            P(),
            P("sp", None),
            P("sp", None),
            P("sp", None, "tp"),
            P("sp", None, "tp"),
            P("sp", "tp", None),
            P(None, "tp"),
            P(None, "tp"),
            P("tp", None),
        ),
        out_specs=P(("sp", "tp"), None),
        check_vma=False,
    )
```

```python
import functools

import jax
import jax.numpy as jnp
from jax import lax
from jax.experimental import pallas as pl
from jax.experimental.pallas import tpu as pltpu
from jax.sharding import PartitionSpec as P

F32 = jnp.float32
BF16 = jnp.bfloat16
CAP = 4
TP = 4
NEAR = 3
NEAR_STEP = 4


def remote(src, dst, send_sem, recv_sem, sp, tp):
    return pltpu.make_async_remote_copy(
        src_ref=src,
        dst_ref=dst,
        send_sem=send_sem,
        recv_sem=recv_sem,
        device_id=(sp, tp),
        device_id_type=pl.DeviceIdType.MESH,
    )


def add_into(dst, src):
    dst[...] = (dst[...].astype(F32) + src[...].astype(F32)).astype(BF16)


def kernel(
    groups,
    resid_h, cb_h, cc_h, cx_h, taps, ow_h, gain, routes, rweight,
    wg_h, wu_h, wd_h, sg_h, su_h, sd_h,
    out,
    resid, cb, cc, cx, ow, wg, wu, wd, sg, su, sd,
    prod, mixed, halo, halo_in, own, proj, proj1, proj2, raw, nrm,
    part, part1, part2, partf,
    rowform, colform, disp, wcomb, outgoing, arr, res, res1, res2, summed, ret,
    near_disp, near_w, near_out, near_arr, near_res, near_ret,
    load_sem, halo_sem, proj_s, proj_r, nrm_s, nrm_r, part_s, part_r,
    a2a_s, a2a_r, ag_s, ag_r, rs_s, rs_r, back_s, back_r, out_s, out_r, home_s, home_r, known,
):
    s = lax.axis_index("sp")
    x = lax.axis_index("tp")
    sp_count = lax.axis_size("sp")
    zs = sp_count // groups
    far = zs - NEAR
    half = groups // 2
    q, d_model = resid.shape
    dh = d_model // 2
    dq = d_model // 4
    toks = cc.shape[0]
    msg = TP * CAP
    right = lax.rem(x + 1, TP)
    left = lax.rem(x + TP - 1, TP)
    z = lax.div(s, groups)
    g = lax.rem(s, groups)

    def sp_ahead(dz, dg):
        return lax.rem(z + dz, zs) * groups + lax.rem(g + dg, groups)

    def sp_behind(dz, dg):
        return lax.rem(z + zs - dz, zs) * groups + lax.rem(g + groups - dg, groups)

    order = sorted(range(2, zs - 1), key=lambda dz: (min(dz, zs - dz) == 2, min(dz, zs - dz)))

    def zone(i):
        dz = order[0]
        for n, other in enumerate(order[1:]):
            dz = jnp.where(i == n + 1, other, dz)
        return dz

    def near_zone(k):
        return jnp.where(k == 0, 1, jnp.where(k == 1, zs - 1, 0))

    pairs = (
        (cc_h, cc), (cx_h, cx), (cb_h, cb), (ow_h, ow), (resid_h, resid),
        (sg_h, sg), (su_h, su), (sd_h, sd), (wg_h.at[0], wg), (wu_h.at[0], wu), (wd_h.at[0], wd),
    )
    loads = [pltpu.make_async_copy(a, b, load_sem.at[i]) for i, (a, b) in enumerate(pairs)]
    for one in loads:
        one.start()

    barrier = pltpu.get_barrier_semaphore()

    def tell(sem, sp, tp):
        pl.semaphore_signal(
            sem, inc=1, device_id=(sp, tp), device_id_type=pl.DeviceIdType.MESH
        )

    core = z * groups + g + 1 - 2 * lax.rem(g, 2)
    y_sides = (sp_ahead(0, 2), sp_behind(0, 2)) if groups > 2 else ()
    z_sides = (sp_ahead(1, 0), sp_behind(1, 0))
    ring_sides = (lax.rem(s + 1, sp_count), lax.rem(s + sp_count - 1, sp_count))
    for side in (right, left):
        tell(barrier, s, side)
    for side in ring_sides + (core,) + y_sides + z_sides:
        tell(barrier, side, x)
    n_near = 2 + 3 + len(y_sides) + 2
    rounds = [(core,)] + [y_sides] * (groups // 4) + [z_sides] * (zs // 2)

    def pass_on(k):
        if k < len(rounds):
            for side in rounds[k]:
                tell(known.at[k], side, x)

    def learn(k):
        if k < len(rounds):
            pl.semaphore_wait(known.at[k], len(rounds[k]))

    for i in range(3):
        loads[i].wait()
    prod[0:8] = jnp.zeros((8, prod.shape[1]), F32)
    prod[8 : 8 + toks] = cc[...].astype(F32) * cx[...].astype(F32)
    halo[...] = prod[toks : toks + 8]

    def mix(n):
        conv = prod[6 : 6 + n] * taps[0:1].astype(F32)
        conv = conv + prod[7 : 7 + n] * taps[1:2].astype(F32)
        conv = conv + prod[8 : 8 + n] * taps[2:3].astype(F32)
        mixed[0:n] = (cb[0:n].astype(F32) * conv).astype(BF16)

    def project(j):
        block = lax.rem(x + TP - j, TP)
        return mixed[pl.ds(pl.multiple_of(block * q, 16), q)]

    mix(toks)
    loads[3].wait()
    for n in range(4):
        for j in (2, 3, 1):
            proj[n // 2, j, n % 2] = jnp.dot(
                project(j), ow[:, n * dq : (n + 1) * dq], preferred_element_type=F32
            ).astype(BF16)

    pl.semaphore_wait(barrier, n_near)
    pass_on(0)
    halo_copy = remote(
        halo, halo_in, halo_sem.at[0], halo_sem.at[1], lax.rem(s + 1, sp_count), x
    )
    halo_copy.start()

    def ring_sum(b, b1, b2, ssem, rsem):
        def far_side():
            remote(b.at[2, 0], b1.at[0], ssem, rsem(0), s, right).start()
            remote(b.at[2, 1], b1.at[1], ssem, rsem(1), s, left).start()

        def to_right():
            remote(b.at[3, 1], b2.at[0, 1], ssem, rsem(2), s, right).start()

        def to_left():
            remote(b.at[1, 0], b2.at[1, 0], ssem, rsem(3), s, left).start()

        def begin():
            far_side()
            to_right()
            to_left()

        def turn():
            remote(b.at[2, 0], b1.at[0], ssem, rsem(0), s, left).wait_recv()
            add_into(b.at[3, 0], b1.at[0])
            remote(b.at[3, 0], b2.at[0, 0], ssem, rsem(4), s, right).start()
            remote(b.at[2, 1], b1.at[1], ssem, rsem(1), s, right).wait_recv()
            add_into(b.at[1, 1], b1.at[1])
            remote(b.at[1, 1], b2.at[1, 1], ssem, rsem(5), s, left).start()

        def finish():
            remote(b.at[3, 1], b2.at[0, 1], ssem, rsem(2), s, left).wait_recv()
            remote(b.at[1, 0], b2.at[1, 0], ssem, rsem(3), s, right).wait_recv()
            remote(b.at[3, 0], b2.at[0, 0], ssem, rsem(4), s, left).wait_recv()
            remote(b.at[1, 1], b2.at[1, 1], ssem, rsem(5), s, right).wait_recv()

        def drain():
            remote(b.at[0:3], b.at[0:3], ssem, rsem(0), s, right).wait_send()

        return begin, turn, finish, drain, (far_side, to_right, to_left)

    def ring_gather(b, ssem, rsem):
        def begin():
            remote(b.at[0], b.at[1], ssem, rsem(0), s, right).start()
            remote(b.at[0], b.at[3], ssem, rsem(1), s, left).start()

        def turn():
            remote(b.at[0], b.at[1], ssem, rsem(0), s, left).wait_recv()
            remote(b.at[1, 0], b.at[2, 0], ssem, rsem(2), s, right).start()
            remote(b.at[0], b.at[3], ssem, rsem(1), s, right).wait_recv()
            remote(b.at[3, 1], b.at[2, 1], ssem, rsem(3), s, left).start()

        def finish():
            remote(b.at[1, 0], b.at[2, 0], ssem, rsem(2), s, left).wait_recv()
            remote(b.at[3, 1], b.at[2, 1], ssem, rsem(3), s, right).wait_recv()

        def drain():
            remote(b.at[0:3], b.at[0:3], ssem, rsem(0), s, right).wait_send()

        return begin, turn, finish, drain

    sums = [
        ring_sum(
            proj.at[c], proj1.at[c], proj2.at[c], proj_s.at[c], lambda k, c=c: proj_r.at[c, k]
        )
        for c in range(2)
    ]
    gathers = [
        ring_gather(raw.at[c], nrm_s.at[c], lambda k, c=c: nrm_r.at[c, k]) for c in range(2)
    ]

    for c in range(2):
        pl.when(x != 2)(sums[c][4][0])
        pl.when(x < 2)(sums[c][4][1])
        pl.when((x == 0) | (x == 3))(sums[c][4][2])

    learn(0)
    pass_on(1)
    halo_copy.wait_recv()
    prod[0:8] = halo_in[...] * jnp.where(s == 0, 0.0, 1.0)
    mix(16)
    for n in range(4):
        proj[n // 2, x, n % 2, 0:16] = jnp.dot(
            mixed[0:16], ow[:, n * dq : (n + 1) * dq], preferred_element_type=F32
        ).astype(BF16)
    for c in range(2):
        pl.when(x == 2)(sums[c][4][0])
        pl.when(x >= 2)(sums[c][4][1])
        pl.when((x == 1) | (x == 2))(sums[c][4][2])
    learn(1)
    pass_on(2)
    for n in range(4):
        own[n // 2, n % 2] = jnp.dot(
            project(0), ow[:, n * dq : (n + 1) * dq], preferred_element_type=F32
        )
    learn(2)
    pass_on(3)

    rowform[0:2] = routes[...].astype(F32)
    rowform[2:4] = rweight[...]
    colform[...] = rowform[...].T
    before = lax.broadcasted_iota(jnp.int32, (q, q), 0) > lax.broadcasted_iota(
        jnp.int32, (q, q), 1
    )
    earlier = jnp.where(before, 1.0, 0.0).astype(BF16)

    def table(j, dz, dg, rank, extra):
        expert = lax.rem(dz + z, zs) * groups + lax.rem(dg + g, groups)
        expert = expert.astype(F32)
        rows = pl.ds(pl.multiple_of(lax.rem(x + TP - j, TP) * q, 16), q)
        is_0 = expert == colform[rows, 0:1]
        named = jnp.where(is_0 | (expert == colform[rows, 1:2]), 1.0, 0.0)
        count = jnp.dot(earlier, named.astype(BF16), preferred_element_type=F32)
        held = jnp.where((count == rank.astype(F32)) & extra, named, 0.0)
        weight = jnp.where(is_0, colform[rows, 2:3], colform[rows, 3:4]) * held
        high = weight.astype(BF16)
        return held.T.astype(BF16), high, (weight - high.astype(F32)).astype(BF16)

    far_slots = far * groups * CAP
    i_slot = lax.broadcasted_iota(jnp.int32, (q, far_slots), 1)
    offset = lax.div(i_slot, CAP)
    disp[...], wcomb[0:q], wcomb[q : 2 * q] = table(
        0, zone(lax.div(offset, groups)), lax.rem(offset, groups), lax.rem(i_slot, CAP),
        i_slot >= 0,
    )

    learn(3)
    pass_on(4)
    sums[0][1]()
    sums[1][1]()

    def settle(c):
        sums[c][2]()
        for h in range(2):
            n = 2 * c + h
            total = own[c, h] + proj2[c, 0, h].astype(F32) + proj2[c, 1, h].astype(F32)
            total = total + resid[:, n * dq : (n + 1) * dq].astype(F32)
            raw[c, 0, h] = total.astype(BF16)
        gathers[c][0]()

    def normalize(j):
        square = jnp.zeros((q, 1), F32)
        for n in range(4):
            m = raw[n // 2, j, n % 2].astype(F32)
            square = square + jnp.sum(m * m, axis=-1, keepdims=True)
        scale = lax.rsqrt(square * (1.0 / d_model) + 1e-06)
        for n in range(4):
            m = raw[n // 2, j, n % 2].astype(F32)
            nrm[n, j] = (m * scale * gain[:, n * dq : (n + 1) * dq]).astype(BF16)

    near_slots = NEAR * groups * msg
    n_slot = lax.broadcasted_iota(jnp.int32, (q, near_slots), 1)
    near_offset = lax.div(n_slot, msg)
    b_slot = lax.broadcasted_iota(jnp.int32, (q, NEAR * groups * CAP), 1)
    b_offset = lax.div(b_slot, CAP)
    for j in range(TP):
        high, low = pl.ds(j * q, q), pl.ds((TP + j) * q, q)
        _, near_w[high], near_w[low] = table(
            j, near_zone(lax.div(near_offset, groups)), lax.rem(near_offset, groups),
            lax.rem(n_slot, CAP), lax.rem(lax.div(n_slot, CAP), TP) == j,
        )
        near_disp[j], _, _ = table(
            j, near_zone(lax.div(b_offset, groups)), lax.rem(b_offset, groups),
            lax.rem(b_slot, CAP), b_slot >= 0,
        )
        learn(4 + j)
        pass_on(5 + j)
        if j == 1:
            loads[4].wait()
            settle(0)

    settle(1)
    normalize(0)

    zone_rows = groups * CAP

    def far_dispatch(low, high):
        @pl.loop(low, high)
        def _(i):
            rows = disp[pl.ds(pl.multiple_of(i * zone_rows, zone_rows), zone_rows)]
            for n in range(4):
                picked = jnp.dot(rows, nrm[n, 0], preferred_element_type=F32)
                outgoing[i, :, :, :, n * dq : (n + 1) * dq] = picked.astype(BF16).reshape(
                    2, half, CAP, dq
                )
            for dg in range(groups):
                remote(
                    outgoing.at[i, dg // half, dg % half], arr.at[i, 0, dg // half, dg % half],
                    a2a_s.at[i], a2a_r.at[i], sp_ahead(zone(i), dg), x,
                ).start()

    near_rows = groups * msg

    def near_dispatch(j):
        for n in range(4):
            picked = jnp.dot(near_disp[j], nrm[n, j], preferred_element_type=F32)
            near_out[:, :, j, :, n * dq : (n + 1) * dq] = picked.astype(BF16).reshape(
                NEAR, groups, CAP, dq
            )

        @pl.loop(0, NEAR)
        def _(k):
            for dg in range(groups):
                @pl.when((k != NEAR - 1) | (dg != 0))
                def _():
                    remote(
                        near_out.at[k, dg, j], near_arr.at[k, dg, j], out_s.at[k], out_r.at[k],
                        sp_ahead(near_zone(k), dg), x,
                    ).start()

    later = min(3, far)
    far_dispatch(0, later)
    near_dispatch(0)
    for one in loads[5:]:
        one.wait()
    gathers[0][1]()
    gathers[1][1]()
    normalize(1)
    normalize(3)
    far_dispatch(later, far)
    near_dispatch(1)
    near_dispatch(3)

    def near_send(src, dst, k, ssem, rsem, target):
        for dg in range(groups):
            @pl.when((k != NEAR - 1) | (dg != 0))
            def _():
                rows = slice(dg * msg, (dg + 1) * msg)
                remote(
                    src.at[k, rows], dst.at[k, rows], ssem.at[k], rsem.at[k],
                    target(near_zone(k), dg), x,
                ).start()

    def near_wait(k, ssem, rsem, recv):
        def fire(a):
            one = remote(a, a, ssem.at[k], rsem.at[k], s, right)
            if recv:
                one.wait_recv()
            else:
                one.wait_send()

        @pl.when(k != NEAR - 1)
        def _():
            fire(near_res.at[k])

        @pl.when(k == NEAR - 1)
        def _():
            fire(near_res.at[k, msg:near_rows])

    def chain(i):
        return ring_sum(res.at[i], res1.at[i], res2.at[i], rs_s.at[i], lambda k: rs_r.at[i, k])

    def spread(i):
        return ring_gather(arr.at[i], ag_s.at[i], lambda k: ag_r.at[i, k])

    n_rows = TP * groups * CAP
    kc = min(256, d_model)
    nc = dq

    def expert(read, write):
        gate = jnp.zeros((n_rows, wg.shape[1]), F32)
        up = jnp.zeros((n_rows, wg.shape[1]), F32)
        for k in range(d_model // kc):
            cols = slice(k * kc, (k + 1) * kc)
            block = read(cols)
            gate = gate + jnp.dot(block, wg[cols], preferred_element_type=F32)
            up = up + jnp.dot(block, wu[cols], preferred_element_type=F32)
        hidden = (jax.nn.silu(gate) * up).astype(BF16)
        for n in range(d_model // nc):
            cols = slice(n * nc, (n + 1) * nc)
            write(cols, jnp.dot(hidden, wd[:, cols], preferred_element_type=F32).astype(BF16))

    def far_expert(i):
        def write(cols, value):
            res[i, :, :, :, :, cols] = value.reshape(TP, 2, half, CAP, nc)

        expert(lambda cols: arr[i, :, :, :, :, cols].reshape(n_rows, kc), write)

    def near_expert(k):
        def write(cols, value):
            near_res[k, :, cols] = value

        expert(lambda cols: near_arr[k, :, :, :, cols].reshape(n_rows, kc), write)

    part_begin, part_turn, part_finish, part_drain, _ = ring_sum(
        part, part1, part2, part_s, lambda k: part_r.at[k]
    )

    def shared():
        gate = jnp.zeros((TP * q, sg.shape[1]), F32)
        up = jnp.zeros((TP * q, sg.shape[1]), F32)
        for n in range(4):
            block = nrm[n].reshape(TP * q, dq)
            gate = gate + jnp.dot(block, sg[n * dq : (n + 1) * dq], preferred_element_type=F32)
            up = up + jnp.dot(block, su[n * dq : (n + 1) * dq], preferred_element_type=F32)
        hidden = (jax.nn.silu(gate) * up).astype(BF16)
        for h in range(2):
            partf[:, h] = jnp.dot(
                hidden, sd[:, h * dh : (h + 1) * dh], preferred_element_type=F32
            ).reshape(TP, q, dh)

    def near_combine():
        for n in range(d_model // kc):
            h, c = divmod(n * kc, dh)
            block = near_ret[:, :, n * kc : (n + 1) * kc].reshape(near_slots, kc)
            both = jnp.dot(near_w[...], block, preferred_element_type=F32)
            total = partf[:, h, :, c : c + kc] + (both[: TP * q] + both[TP * q :]).reshape(
                TP, q, kc
            )
            part[:, h, :, c : c + kc] = total.astype(BF16)

    def far_combine():
        for n in range(d_model // nc):
            h, c = divmod(n * nc, dh)
            block = ret[:, :, :, :, n * nc : (n + 1) * nc].reshape(far_slots, nc)
            both = jnp.dot(wcomb[...], block, preferred_element_type=F32)
            own[n // 2, n % 2] = (
                both[:q] + both[q:] + raw[n // 2, 0, n % 2].astype(F32)
                + part[0, h, :, c : c + nc].astype(F32)
            )

    @pl.loop(0, far + 4)
    def _(i):
        @pl.when(i < far)
        def _():
            a = arr.at[i, 0]
            remote(a, a, a2a_s.at[i], a2a_r.at[i], s, right).wait_recv()
            spread(i)[0]()

        @pl.when(i == NEAR_STEP)
        def _():
            @pl.loop(0, NEAR)
            def _(k):
                near_wait(k, out_s, out_r, True)
                near_expert(k)
                near_send(near_res, near_ret, k, home_s, home_r, sp_behind)

        @pl.when(i == 0)
        def _():
            gathers[0][2]()
            gathers[1][2]()
            normalize(2)
            near_dispatch(2)
            near_arr[NEAR - 1, 0] = near_out[NEAR - 1, 0]

        @pl.when((i >= 1) & (i < far + 1))
        def _():
            spread(i - 1)[1]()

        @pl.when(i == 1)
        def _():
            shared()

        @pl.when((i >= 2) & (i < far + 2))
        def _():
            spread(i - 2)[2]()
            far_expert(i - 2)
            chain(i - 2)[0]()

        @pl.when((i >= 3) & (i < far + 3))
        def _():
            chain(i - 3)[1]()

        @pl.when(i == far + 3)
        def _():
            near_ret[NEAR - 1, 0:msg] = near_res[NEAR - 1, 0:msg]
            for k in range(NEAR):
                near_wait(k, home_s, home_r, True)
            near_combine()
            part_begin()

        @pl.when((i >= 4) & (i < far + 4))
        def _():
            k = i - 4
            chain(k)[2]()
            summed[k] = (
                res[k, 0].astype(F32) + res2[k, 0].astype(F32) + res2[k, 1].astype(F32)
            ).astype(BF16)
            for dg in range(groups):
                remote(
                    summed.at[k, dg // half, dg % half], ret.at[k, dg // half, dg % half],
                    back_s.at[k], back_r.at[k], sp_behind(zone(k), dg), x,
                ).start()

    part_turn()

    @pl.loop(0, far)
    def _(i):
        a = ret.at[i]
        remote(a, a, back_s.at[i], back_r.at[i], s, right).wait_recv()

    far_combine()
    part_finish()
    for n in range(4):
        h, c = divmod(n * dq, dh)
        total = own[n // 2, n % 2] + part2[0, h, :, c : c + dq].astype(F32)
        total = total + part2[1, h, :, c : c + dq].astype(F32)
        out[:, n * dq : (n + 1) * dq] = total.astype(BF16)

    halo_copy.wait_send()
    for c in range(2):
        sums[c][3]()
        gathers[c][3]()
    part_drain()

    @pl.loop(0, far)
    def _(i):
        a = outgoing.at[i]
        remote(a, a, a2a_s.at[i], a2a_r.at[i], s, right).wait_send()
        b = summed.at[i]
        remote(b, b, back_s.at[i], back_r.at[i], s, right).wait_send()
        spread(i)[3]()
        chain(i)[3]()

    for k in range(NEAR):
        near_wait(k, out_s, out_r, False)
        near_wait(k, home_s, home_r, False)


def local(
    resid, conv_b, conv_c, conv_x, conv_taps, out_weight, norm_gain, routes, route_weight,
    expert_gate, expert_up, expert_down, shared_gate, shared_up, shared_down,
):
    sp_count = lax.axis_size("sp")
    groups = max(2, sp_count // 8)
    zs = sp_count // groups
    half = groups // 2
    far = zs - NEAR
    near_slots = NEAR * groups * TP * CAP
    q, d = resid.shape
    toks, ch = conv_b.shape
    ff = expert_gate.shape[2]
    dh = d // 2
    dq = d // 4
    vmem = pltpu.VMEM
    dma = pltpu.SemaphoreType.DMA
    anywhere = pl.BlockSpec(memory_space=pl.ANY)
    inside = pl.BlockSpec(memory_space=pltpu.VMEM)
    return pl.pallas_call(
        functools.partial(kernel, groups),
        out_shape=jax.ShapeDtypeStruct((q, d), BF16),
        in_specs=[anywhere] * 4 + [inside, anywhere] + [inside] * 3 + [anywhere] * 6,
        out_specs=inside,
        scratch_shapes=[
            vmem((q, d), BF16), vmem((toks, ch), BF16), vmem((toks, ch), BF16),
            vmem((toks, ch), BF16), vmem((ch, d), BF16),
            vmem((d, ff), BF16), vmem((d, ff), BF16), vmem((ff, d), BF16),
            vmem((d, ff), BF16), vmem((d, ff), BF16), vmem((ff, d), BF16),
            vmem((toks + 8, ch), F32), vmem((toks, ch), BF16), vmem((8, ch), F32), vmem((8, ch), F32),
            vmem((2, 2, q, dq), F32),
            vmem((2, 4, 2, q, dq), BF16), vmem((2, 2, q, dq), BF16),
            vmem((2, 2, 2, q, dq), BF16),
            vmem((2, 4, 2, q, dq), BF16), vmem((4, 4, q, dq), BF16),
            vmem((4, 2, q, dh), BF16), vmem((2, q, dh), BF16), vmem((2, 2, q, dh), BF16),
            vmem((4, 2, q, dh), F32),
            vmem((8, toks), F32), vmem((toks, 8), F32),
            vmem((far * groups * CAP, q), BF16), vmem((2 * q, far * groups * CAP), BF16),
            vmem((far, 2, half, CAP, d), BF16),
            vmem((far, 4, 2, half, CAP, d), BF16),
            vmem((far, 4, 2, half, CAP, d), BF16),
            vmem((far, 2, half, CAP, d), BF16),
            vmem((far, 2, 2, half, CAP, d), BF16),
            vmem((far, 2, half, CAP, d), BF16),
            vmem((far, 2, half, CAP, d), BF16),
            vmem((TP, NEAR * groups * CAP, q), BF16), vmem((2 * TP * q, near_slots), BF16),
            vmem((NEAR, groups, TP, CAP, d), BF16), vmem((NEAR, groups, TP, CAP, d), BF16),
            vmem((NEAR, groups * TP * CAP, d), BF16), vmem((NEAR, groups * TP * CAP, d), BF16),
            dma((11,)), dma((2,)), dma((2,)), dma((2, 6)), dma((2,)), dma((2, 4)), dma(()), dma((6,)),
            dma((far,)), dma((far,)), dma((far,)), dma((far, 4)), dma((far,)), dma((far, 6)),
            dma((far,)), dma((far,)), dma((NEAR,)), dma((NEAR,)), dma((NEAR,)), dma((NEAR,)),
            pltpu.SemaphoreType.REGULAR((8,)),
        ],
        compiler_params=pltpu.CompilerParams(
            collective_id=0, has_side_effects=True, vmem_limit_bytes=60 * 1024 * 1024
        ),
        name="layer",
    )(
        resid, conv_b, conv_c, conv_x, conv_taps, out_weight, norm_gain.reshape(1, d), routes.T,
        route_weight.T, expert_gate, expert_up, expert_down, shared_gate, shared_up, shared_down,
    )


def solution(mesh):
    return jax.shard_map(
        local,
        mesh=mesh,
        in_specs=(
            P(("sp", "tp"), None),
            P("sp", "tp"),
            P("sp", "tp"),
            P("sp", "tp"),
            P(None, "tp"),
            P("tp", None),
            P(),
            P("sp", None),
            P("sp", None),
            P("sp", None, "tp"),
            P("sp", None, "tp"),
            P("sp", "tp", None),
            P(None, "tp"),
            P(None, "tp"),
            P("tp", None),
        ),
        out_specs=P(("sp", "tp"), None),
        check_vma=False,
    )
```

```python
import functools

import jax
import jax.numpy as jnp
from jax import lax
from jax.experimental import pallas as pl
from jax.experimental.pallas import tpu as pltpu
from jax.sharding import PartitionSpec as P

F32 = jnp.float32
BF16 = jnp.bfloat16
CAP = 4
TP = 4
NEAR = 3
NEAR_STEP = 4


def remote(src, dst, send_sem, recv_sem, sp, tp):
    return pltpu.make_async_remote_copy(
        src_ref=src,
        dst_ref=dst,
        send_sem=send_sem,
        recv_sem=recv_sem,
        device_id=(sp, tp),
        device_id_type=pl.DeviceIdType.MESH,
    )


def add_into(dst, src):
    dst[...] = (dst[...].astype(F32) + src[...].astype(F32)).astype(BF16)


def kernel(
    groups,
    resid_h, cb_h, cc_h, cx_h, taps, ow_h, gain, routes, rweight,
    wg_h, wu_h, wd_h, sg_h, su_h, sd_h,
    out,
    resid, cb, cc, cx, ow, wg, wu, wd, sg, su, sd,
    prod, mixed, halo, halo_in, own, proj, proj1, proj2, raw, nrm,
    part, part1, part2, partf,
    rowform, colform, disp, wcomb, outgoing, arr, res, res1, res2, summed, ret,
    near_disp, near_w, near_out, near_arr, near_res, near_ret,
    load_sem, halo_sem, proj_s, proj_r, nrm_s, nrm_r, part_s, part_r,
    a2a_s, a2a_r, ag_s, ag_r, rs_s, rs_r, back_s, back_r, out_s, out_r, home_s, home_r, known,
):
    s = lax.axis_index("sp")
    x = lax.axis_index("tp")
    sp_count = lax.axis_size("sp")
    zs = sp_count // groups
    far = zs - NEAR
    half = groups // 2
    q, d_model = resid.shape
    dh = d_model // 2
    dq = d_model // 4
    toks = cc.shape[0]
    msg = TP * CAP
    right = lax.rem(x + 1, TP)
    left = lax.rem(x + TP - 1, TP)
    z = lax.div(s, groups)
    g = lax.rem(s, groups)

    def sp_ahead(dz, dg):
        return lax.rem(z + dz, zs) * groups + lax.rem(g + dg, groups)

    def sp_behind(dz, dg):
        return lax.rem(z + zs - dz, zs) * groups + lax.rem(g + groups - dg, groups)

    order = sorted(range(2, zs - 1), key=lambda dz: (min(dz, zs - dz) == 2, min(dz, zs - dz)))

    def zone(i):
        dz = order[0]
        for n, other in enumerate(order[1:]):
            dz = jnp.where(i == n + 1, other, dz)
        return dz

    def near_zone(k):
        return jnp.where(k == 0, 1, jnp.where(k == 1, zs - 1, 0))

    pairs = (
        (cc_h, cc), (cx_h, cx), (cb_h, cb), (ow_h, ow), (resid_h, resid),
        (sg_h, sg), (su_h, su), (sd_h, sd), (wg_h.at[0], wg), (wu_h.at[0], wu), (wd_h.at[0], wd),
    )
    loads = [pltpu.make_async_copy(a, b, load_sem.at[i]) for i, (a, b) in enumerate(pairs)]
    for one in loads:
        one.start()

    barrier = pltpu.get_barrier_semaphore()

    def tell(sem, sp, tp):
        pl.semaphore_signal(
            sem, inc=1, device_id=(sp, tp), device_id_type=pl.DeviceIdType.MESH
        )

    core = z * groups + g + 1 - 2 * lax.rem(g, 2)
    y_sides = (sp_ahead(0, 2), sp_behind(0, 2)) if groups > 2 else ()
    z_sides = (sp_ahead(1, 0), sp_behind(1, 0))
    ring_sides = (lax.rem(s + 1, sp_count), lax.rem(s + sp_count - 1, sp_count))
    for side in (right, left):
        tell(barrier, s, side)
    for side in ring_sides + (core,) + y_sides + z_sides:
        tell(barrier, side, x)
    n_near = 2 + 3 + len(y_sides) + 2
    rounds = [(core,)] + [y_sides] * (groups // 4) + [z_sides] * (zs // 2)

    def pass_on(k):
        if k < len(rounds):
            for side in rounds[k]:
                tell(known.at[k], side, x)

    def learn(k):
        if k < len(rounds):
            pl.semaphore_wait(known.at[k], len(rounds[k]))

    for i in range(3):
        loads[i].wait()
    prod[0:8] = jnp.zeros((8, prod.shape[1]), F32)
    prod[8 : 8 + toks] = cc[...].astype(F32) * cx[...].astype(F32)
    halo[...] = prod[toks : toks + 8]

    def mix(n):
        conv = prod[6 : 6 + n] * taps[0:1].astype(F32)
        conv = conv + prod[7 : 7 + n] * taps[1:2].astype(F32)
        conv = conv + prod[8 : 8 + n] * taps[2:3].astype(F32)
        mixed[0:n] = (cb[0:n].astype(F32) * conv).astype(BF16)

    def project(j):
        block = lax.rem(x + TP - j, TP)
        return mixed[pl.ds(pl.multiple_of(block * q, 16), q)]

    mix(toks)
    loads[3].wait()
    for n in range(4):
        for j in (2, 3, 1):
            proj[n // 2, j, n % 2] = jnp.dot(
                project(j), ow[:, n * dq : (n + 1) * dq], preferred_element_type=F32
            ).astype(BF16)

    pl.semaphore_wait(barrier, n_near)
    pass_on(0)
    halo_copy = remote(
        halo, halo_in, halo_sem.at[0], halo_sem.at[1], lax.rem(s + 1, sp_count), x
    )
    halo_copy.start()

    def ring_sum(b, b1, b2, ssem, rsem):
        def far_side():
            remote(b.at[2, 0], b1.at[0], ssem, rsem(0), s, right).start()
            remote(b.at[2, 1], b1.at[1], ssem, rsem(1), s, left).start()

        def to_right():
            remote(b.at[3, 1], b2.at[0, 1], ssem, rsem(2), s, right).start()

        def to_left():
            remote(b.at[1, 0], b2.at[1, 0], ssem, rsem(3), s, left).start()

        def begin():
            far_side()
            to_right()
            to_left()

        def turn():
            remote(b.at[2, 0], b1.at[0], ssem, rsem(0), s, left).wait_recv()
            add_into(b.at[3, 0], b1.at[0])
            remote(b.at[3, 0], b2.at[0, 0], ssem, rsem(4), s, right).start()
            remote(b.at[2, 1], b1.at[1], ssem, rsem(1), s, right).wait_recv()
            add_into(b.at[1, 1], b1.at[1])
            remote(b.at[1, 1], b2.at[1, 1], ssem, rsem(5), s, left).start()

        def finish():
            remote(b.at[3, 1], b2.at[0, 1], ssem, rsem(2), s, left).wait_recv()
            remote(b.at[1, 0], b2.at[1, 0], ssem, rsem(3), s, right).wait_recv()
            remote(b.at[3, 0], b2.at[0, 0], ssem, rsem(4), s, left).wait_recv()
            remote(b.at[1, 1], b2.at[1, 1], ssem, rsem(5), s, right).wait_recv()

        def drain():
            remote(b.at[0:3], b.at[0:3], ssem, rsem(0), s, right).wait_send()

        return begin, turn, finish, drain, (far_side, to_right, to_left)

    def ring_gather(b, ssem, rsem):
        def begin():
            remote(b.at[0], b.at[1], ssem, rsem(0), s, right).start()
            remote(b.at[0], b.at[3], ssem, rsem(1), s, left).start()

        def turn():
            remote(b.at[0], b.at[1], ssem, rsem(0), s, left).wait_recv()
            remote(b.at[1, 0], b.at[2, 0], ssem, rsem(2), s, right).start()
            remote(b.at[0], b.at[3], ssem, rsem(1), s, right).wait_recv()
            remote(b.at[3, 1], b.at[2, 1], ssem, rsem(3), s, left).start()

        def finish():
            remote(b.at[1, 0], b.at[2, 0], ssem, rsem(2), s, left).wait_recv()
            remote(b.at[3, 1], b.at[2, 1], ssem, rsem(3), s, right).wait_recv()

        def drain():
            remote(b.at[0:3], b.at[0:3], ssem, rsem(0), s, right).wait_send()

        return begin, turn, finish, drain

    sums = [
        ring_sum(
            proj.at[c], proj1.at[c], proj2.at[c], proj_s.at[c], lambda k, c=c: proj_r.at[c, k]
        )
        for c in range(2)
    ]
    gathers = [
        ring_gather(raw.at[c], nrm_s.at[c], lambda k, c=c: nrm_r.at[c, k]) for c in range(2)
    ]

    for c in range(2):
        pl.when(x != 2)(sums[c][4][0])
        pl.when(x < 2)(sums[c][4][1])
        pl.when((x == 0) | (x == 3))(sums[c][4][2])

    learn(0)
    pass_on(1)
    halo_copy.wait_recv()
    prod[0:8] = halo_in[...] * jnp.where(s == 0, 0.0, 1.0)
    mix(16)
    for n in range(4):
        proj[n // 2, x, n % 2, 0:16] = jnp.dot(
            mixed[0:16], ow[:, n * dq : (n + 1) * dq], preferred_element_type=F32
        ).astype(BF16)
    for c in range(2):
        pl.when(x == 2)(sums[c][4][0])
        pl.when(x >= 2)(sums[c][4][1])
        pl.when((x == 1) | (x == 2))(sums[c][4][2])
    learn(1)
    pass_on(2)
    for n in range(4):
        own[n // 2, n % 2] = jnp.dot(
            project(0), ow[:, n * dq : (n + 1) * dq], preferred_element_type=F32
        )
    learn(2)
    pass_on(3)

    rowform[0:2] = routes[...].astype(F32)
    rowform[2:4] = rweight[...]
    colform[...] = rowform[...].T
    before = lax.broadcasted_iota(jnp.int32, (q, q), 0) > lax.broadcasted_iota(
        jnp.int32, (q, q), 1
    )
    earlier = jnp.where(before, 1.0, 0.0).astype(BF16)

    def table(j, dz, dg, rank, extra):
        expert = lax.rem(dz + z, zs) * groups + lax.rem(dg + g, groups)
        expert = expert.astype(F32)
        rows = pl.ds(pl.multiple_of(lax.rem(x + TP - j, TP) * q, 16), q)
        is_0 = expert == colform[rows, 0:1]
        named = jnp.where(is_0 | (expert == colform[rows, 1:2]), 1.0, 0.0)
        count = jnp.dot(earlier, named.astype(BF16), preferred_element_type=F32)
        held = jnp.where((count == rank.astype(F32)) & extra, named, 0.0)
        weight = jnp.where(is_0, colform[rows, 2:3], colform[rows, 3:4]) * held
        high = weight.astype(BF16)
        return held.T.astype(BF16), high, (weight - high.astype(F32)).astype(BF16)

    far_slots = far * groups * CAP
    i_slot = lax.broadcasted_iota(jnp.int32, (q, far_slots), 1)
    offset = lax.div(i_slot, CAP)
    disp[...], wcomb[0:q], wcomb[q : 2 * q] = table(
        0, zone(lax.div(offset, groups)), lax.rem(offset, groups), lax.rem(i_slot, CAP),
        i_slot >= 0,
    )

    learn(3)
    pass_on(4)
    sums[0][1]()
    sums[1][1]()

    def settle(c):
        sums[c][2]()
        for h in range(2):
            n = 2 * c + h
            total = own[c, h] + proj2[c, 0, h].astype(F32) + proj2[c, 1, h].astype(F32)
            total = total + resid[:, n * dq : (n + 1) * dq].astype(F32)
            raw[c, 0, h] = total.astype(BF16)
        gathers[c][0]()

    def normalize(j):
        square = jnp.zeros((q, 1), F32)
        for n in range(4):
            m = raw[n // 2, j, n % 2].astype(F32)
            square = square + jnp.sum(m * m, axis=-1, keepdims=True)
        scale = lax.rsqrt(square * (1.0 / d_model) + 1e-06)
        for n in range(4):
            m = raw[n // 2, j, n % 2].astype(F32)
            nrm[n, j] = (m * scale * gain[:, n * dq : (n + 1) * dq]).astype(BF16)

    near_slots = NEAR * groups * msg
    n_slot = lax.broadcasted_iota(jnp.int32, (q, near_slots), 1)
    near_offset = lax.div(n_slot, msg)
    b_slot = lax.broadcasted_iota(jnp.int32, (q, NEAR * groups * CAP), 1)
    b_offset = lax.div(b_slot, CAP)
    for j in range(TP):
        high, low = pl.ds(2 * j * q, q), pl.ds((2 * j + 1) * q, q)
        _, near_w[high], near_w[low] = table(
            j, near_zone(lax.div(near_offset, groups)), lax.rem(near_offset, groups),
            lax.rem(n_slot, CAP), lax.rem(lax.div(n_slot, CAP), TP) == j,
        )
        near_disp[j], _, _ = table(
            j, near_zone(lax.div(b_offset, groups)), lax.rem(b_offset, groups),
            lax.rem(b_slot, CAP), b_slot >= 0,
        )
        learn(4 + j)
        pass_on(5 + j)
        if j == 1:
            loads[4].wait()
            settle(0)

    settle(1)
    normalize(0)

    zone_rows = groups * CAP

    def far_dispatch(low, high):
        @pl.loop(low, high)
        def _(i):
            rows = disp[pl.ds(pl.multiple_of(i * zone_rows, zone_rows), zone_rows)]
            for n in range(4):
                picked = jnp.dot(rows, nrm[n, 0], preferred_element_type=F32)
                outgoing[i, :, :, :, n * dq : (n + 1) * dq] = picked.astype(BF16).reshape(
                    2, half, CAP, dq
                )
            for dg in range(groups):
                remote(
                    outgoing.at[i, dg // half, dg % half], arr.at[i, 0, dg // half, dg % half],
                    a2a_s.at[i], a2a_r.at[i], sp_ahead(zone(i), dg), x,
                ).start()

    near_rows = groups * msg

    def near_dispatch(j):
        for n in range(4):
            picked = jnp.dot(near_disp[j], nrm[n, j], preferred_element_type=F32)
            near_out[:, :, j, :, n * dq : (n + 1) * dq] = picked.astype(BF16).reshape(
                NEAR, groups, CAP, dq
            )

        @pl.loop(0, NEAR)
        def _(k):
            for dg in range(groups):
                @pl.when((k != NEAR - 1) | (dg != 0))
                def _():
                    remote(
                        near_out.at[k, dg, j], near_arr.at[k, dg, j], out_s.at[k], out_r.at[k],
                        sp_ahead(near_zone(k), dg), x,
                    ).start()

    later = min(3, far)
    far_dispatch(0, later)
    near_dispatch(0)
    for one in loads[5:]:
        one.wait()
    gathers[0][1]()
    gathers[1][1]()
    normalize(1)
    normalize(3)
    far_dispatch(later, far)
    near_dispatch(1)
    near_dispatch(3)

    def near_send(src, dst, k, ssem, rsem, target):
        for dg in range(groups):
            @pl.when((k != NEAR - 1) | (dg != 0))
            def _():
                rows = slice(dg * msg, (dg + 1) * msg)
                remote(
                    src.at[k, rows], dst.at[k, rows], ssem.at[k], rsem.at[k],
                    target(near_zone(k), dg), x,
                ).start()

    def near_wait(k, ssem, rsem, recv):
        def fire(a):
            one = remote(a, a, ssem.at[k], rsem.at[k], s, right)
            if recv:
                one.wait_recv()
            else:
                one.wait_send()

        @pl.when(k != NEAR - 1)
        def _():
            fire(near_res.at[k])

        @pl.when(k == NEAR - 1)
        def _():
            fire(near_res.at[k, msg:near_rows])

    def chain(i):
        return ring_sum(res.at[i], res1.at[i], res2.at[i], rs_s.at[i], lambda k: rs_r.at[i, k])

    def spread(i):
        return ring_gather(arr.at[i], ag_s.at[i], lambda k: ag_r.at[i, k])

    n_rows = TP * groups * CAP
    kc = min(256, d_model)
    nc = dq

    def expert(read, write):
        gate = jnp.zeros((n_rows, wg.shape[1]), F32)
        up = jnp.zeros((n_rows, wg.shape[1]), F32)
        for k in range(d_model // kc):
            cols = slice(k * kc, (k + 1) * kc)
            block = read(cols)
            gate = gate + jnp.dot(block, wg[cols], preferred_element_type=F32)
            up = up + jnp.dot(block, wu[cols], preferred_element_type=F32)
        hidden = (jax.nn.silu(gate) * up).astype(BF16)
        for n in range(d_model // nc):
            cols = slice(n * nc, (n + 1) * nc)
            write(cols, jnp.dot(hidden, wd[:, cols], preferred_element_type=F32).astype(BF16))

    def far_expert(i):
        def write(cols, value):
            res[i, :, :, :, :, cols] = value.reshape(TP, 2, half, CAP, nc)

        expert(lambda cols: arr[i, :, :, :, :, cols].reshape(n_rows, kc), write)

    def near_expert(k):
        def write(cols, value):
            near_res[k, :, cols] = value

        expert(lambda cols: near_arr[k, :, :, :, cols].reshape(n_rows, kc), write)

    _, part_turn, part_finish, part_drain, (part_far, part_right, part_left) = ring_sum(
        part, part1, part2, part_s, lambda k: part_r.at[k]
    )

    def shared():
        gate = jnp.zeros((TP * q, sg.shape[1]), F32)
        up = jnp.zeros((TP * q, sg.shape[1]), F32)
        for n in range(4):
            block = nrm[n].reshape(TP * q, dq)
            gate = gate + jnp.dot(block, sg[n * dq : (n + 1) * dq], preferred_element_type=F32)
            up = up + jnp.dot(block, su[n * dq : (n + 1) * dq], preferred_element_type=F32)
        hidden = (jax.nn.silu(gate) * up).astype(BF16)
        for h in range(2):
            partf[:, h] = jnp.dot(
                hidden, sd[:, h * dh : (h + 1) * dh], preferred_element_type=F32
            ).reshape(TP, q, dh)

    def near_combine(j):
        weights = near_w[2 * j * q : 2 * (j + 1) * q]
        for n in range(d_model // nc):
            h, c = divmod(n * nc, dh)
            block = near_ret[:, :, n * nc : (n + 1) * nc].reshape(near_slots, nc)
            both = jnp.dot(weights, block, preferred_element_type=F32)
            total = partf[j, h, :, c : c + nc] + both[:q] + both[q:]
            part[j, h, :, c : c + nc] = total.astype(BF16)

    def far_combine():
        for n in range(d_model // nc):
            h, c = divmod(n * nc, dh)
            block = ret[:, :, :, :, n * nc : (n + 1) * nc].reshape(far_slots, nc)
            both = jnp.dot(wcomb[...], block, preferred_element_type=F32)
            own[n // 2, n % 2] = (
                both[:q] + both[q:] + raw[n // 2, 0, n % 2].astype(F32)
                + part[0, h, :, c : c + nc].astype(F32)
            )

    @pl.loop(0, far + 4)
    def _(i):
        @pl.when(i < far)
        def _():
            a = arr.at[i, 0]
            remote(a, a, a2a_s.at[i], a2a_r.at[i], s, right).wait_recv()
            spread(i)[0]()

        @pl.when(i == NEAR_STEP)
        def _():
            @pl.loop(0, NEAR)
            def _(k):
                near_wait(k, out_s, out_r, True)
                near_expert(k)
                near_send(near_res, near_ret, k, home_s, home_r, sp_behind)

        @pl.when(i == 0)
        def _():
            gathers[0][2]()
            gathers[1][2]()
            normalize(2)
            near_dispatch(2)
            near_arr[NEAR - 1, 0] = near_out[NEAR - 1, 0]

        @pl.when((i >= 1) & (i < far + 1))
        def _():
            spread(i - 1)[1]()

        @pl.when(i == 1)
        def _():
            shared()

        @pl.when((i >= 2) & (i < far + 2))
        def _():
            spread(i - 2)[2]()
            far_expert(i - 2)
            chain(i - 2)[0]()

        @pl.when((i >= 3) & (i < far + 3))
        def _():
            chain(i - 3)[1]()

        @pl.when(i == far + 3)
        def _():
            near_ret[NEAR - 1, 0:msg] = near_res[NEAR - 1, 0:msg]
            for k in range(NEAR):
                near_wait(k, home_s, home_r, True)
            near_combine(2)
            part_far()

        @pl.when((i >= 4) & (i < far + 4))
        def _():
            k = i - 4
            chain(k)[2]()
            summed[k] = (
                res[k, 0].astype(F32) + res2[k, 0].astype(F32) + res2[k, 1].astype(F32)
            ).astype(BF16)
            for dg in range(groups):
                remote(
                    summed.at[k, dg // half, dg % half], ret.at[k, dg // half, dg % half],
                    back_s.at[k], back_r.at[k], sp_behind(zone(k), dg), x,
                ).start()

    near_combine(3)
    part_right()
    near_combine(1)
    part_left()
    near_combine(0)
    part_turn()

    @pl.loop(0, far)
    def _(i):
        a = ret.at[i]
        remote(a, a, back_s.at[i], back_r.at[i], s, right).wait_recv()

    far_combine()
    part_finish()
    for n in range(4):
        h, c = divmod(n * dq, dh)
        total = own[n // 2, n % 2] + part2[0, h, :, c : c + dq].astype(F32)
        total = total + part2[1, h, :, c : c + dq].astype(F32)
        out[:, n * dq : (n + 1) * dq] = total.astype(BF16)

    halo_copy.wait_send()
    for c in range(2):
        sums[c][3]()
        gathers[c][3]()
    part_drain()

    @pl.loop(0, far)
    def _(i):
        a = outgoing.at[i]
        remote(a, a, a2a_s.at[i], a2a_r.at[i], s, right).wait_send()
        b = summed.at[i]
        remote(b, b, back_s.at[i], back_r.at[i], s, right).wait_send()
        spread(i)[3]()
        chain(i)[3]()

    for k in range(NEAR):
        near_wait(k, out_s, out_r, False)
        near_wait(k, home_s, home_r, False)


def local(
    resid, conv_b, conv_c, conv_x, conv_taps, out_weight, norm_gain, routes, route_weight,
    expert_gate, expert_up, expert_down, shared_gate, shared_up, shared_down,
):
    sp_count = lax.axis_size("sp")
    groups = max(2, sp_count // 8)
    zs = sp_count // groups
    half = groups // 2
    far = zs - NEAR
    near_slots = NEAR * groups * TP * CAP
    q, d = resid.shape
    toks, ch = conv_b.shape
    ff = expert_gate.shape[2]
    dh = d // 2
    dq = d // 4
    vmem = pltpu.VMEM
    dma = pltpu.SemaphoreType.DMA
    anywhere = pl.BlockSpec(memory_space=pl.ANY)
    inside = pl.BlockSpec(memory_space=pltpu.VMEM)
    return pl.pallas_call(
        functools.partial(kernel, groups),
        out_shape=pltpu.VMEM((q, d), BF16),
        in_specs=[anywhere] * 4 + [inside, anywhere] + [inside] * 3 + [anywhere] * 6,
        out_specs=inside,
        scratch_shapes=[
            vmem((q, d), BF16), vmem((toks, ch), BF16), vmem((toks, ch), BF16),
            vmem((toks, ch), BF16), vmem((ch, d), BF16),
            vmem((d, ff), BF16), vmem((d, ff), BF16), vmem((ff, d), BF16),
            vmem((d, ff), BF16), vmem((d, ff), BF16), vmem((ff, d), BF16),
            vmem((toks + 8, ch), F32), vmem((toks, ch), BF16), vmem((8, ch), F32), vmem((8, ch), F32),
            vmem((2, 2, q, dq), F32),
            vmem((2, 4, 2, q, dq), BF16), vmem((2, 2, q, dq), BF16),
            vmem((2, 2, 2, q, dq), BF16),
            vmem((2, 4, 2, q, dq), BF16), vmem((4, 4, q, dq), BF16),
            vmem((4, 2, q, dh), BF16), vmem((2, q, dh), BF16), vmem((2, 2, q, dh), BF16),
            vmem((4, 2, q, dh), F32),
            vmem((8, toks), F32), vmem((toks, 8), F32),
            vmem((far * groups * CAP, q), BF16), vmem((2 * q, far * groups * CAP), BF16),
            vmem((far, 2, half, CAP, d), BF16),
            vmem((far, 4, 2, half, CAP, d), BF16),
            vmem((far, 4, 2, half, CAP, d), BF16),
            vmem((far, 2, half, CAP, d), BF16),
            vmem((far, 2, 2, half, CAP, d), BF16),
            vmem((far, 2, half, CAP, d), BF16),
            vmem((far, 2, half, CAP, d), BF16),
            vmem((TP, NEAR * groups * CAP, q), BF16), vmem((2 * TP * q, near_slots), BF16),
            vmem((NEAR, groups, TP, CAP, d), BF16), vmem((NEAR, groups, TP, CAP, d), BF16),
            vmem((NEAR, groups * TP * CAP, d), BF16), vmem((NEAR, groups * TP * CAP, d), BF16),
            dma((11,)), dma((2,)), dma((2,)), dma((2, 6)), dma((2,)), dma((2, 4)), dma(()), dma((6,)),
            dma((far,)), dma((far,)), dma((far,)), dma((far, 4)), dma((far,)), dma((far, 6)),
            dma((far,)), dma((far,)), dma((NEAR,)), dma((NEAR,)), dma((NEAR,)), dma((NEAR,)),
            pltpu.SemaphoreType.REGULAR((8,)),
        ],
        compiler_params=pltpu.CompilerParams(
            collective_id=0, has_side_effects=True, vmem_limit_bytes=60 * 1024 * 1024
        ),
        name="layer",
    )(
        resid, conv_b, conv_c, conv_x, conv_taps, out_weight, norm_gain.reshape(1, d), routes.T,
        route_weight.T, expert_gate, expert_up, expert_down, shared_gate, shared_up, shared_down,
    )


def solution(mesh):
    return jax.shard_map(
        local,
        mesh=mesh,
        in_specs=(
            P(("sp", "tp"), None),
            P("sp", "tp"),
            P("sp", "tp"),
            P("sp", "tp"),
            P(None, "tp"),
            P("tp", None),
            P(),
            P("sp", None),
            P("sp", None),
            P("sp", None, "tp"),
            P("sp", None, "tp"),
            P("sp", "tp", None),
            P(None, "tp"),
            P(None, "tp"),
            P("tp", None),
        ),
        out_specs=P(("sp", "tp"), None),
        check_vma=False,
    )
```

```python
import functools

import jax
import jax.numpy as jnp
from jax import lax
from jax.experimental import pallas as pl
from jax.experimental.pallas import tpu as pltpu
from jax.sharding import PartitionSpec as P

F32 = jnp.float32
BF16 = jnp.bfloat16
CAP = 4
TP = 4
NEAR = 3
NEAR_STEP = 4


def remote(src, dst, send_sem, recv_sem, sp, tp):
    return pltpu.make_async_remote_copy(
        src_ref=src,
        dst_ref=dst,
        send_sem=send_sem,
        recv_sem=recv_sem,
        device_id=(sp, tp),
        device_id_type=pl.DeviceIdType.MESH,
    )


def add_into(dst, src):
    dst[...] = (dst[...].astype(F32) + src[...].astype(F32)).astype(BF16)


def kernel(
    groups,
    resid_h, cb_h, cc_h, cx_h, taps, ow_h, gain, routes, rweight,
    wg_h, wu_h, wd_h, sg_h, su_h, sd_h,
    out,
    resid, cb, cc, cx, ow, wg, wu, wd, sg, su, sd,
    prod, mixed, halo, halo_in, own, proj, proj1, proj2, raw, nrm,
    part, part1, part2, partf,
    rowform, colform, disp, wcomb, outgoing, arr, res, res1, res2, summed, ret,
    near_disp, near_w, near_out, near_arr, near_res, near_ret,
    load_sem, halo_sem, proj_s, proj_r, nrm_s, nrm_r, part_s, part_r,
    a2a_s, a2a_r, ag_s, ag_r, rs_s, rs_r, back_s, back_r, out_s, out_r, home_s, home_r, known,
):
    s = lax.axis_index("sp")
    x = lax.axis_index("tp")
    sp_count = lax.axis_size("sp")
    zs = sp_count // groups
    far = zs - NEAR
    half = groups // 2
    q, d_model = resid.shape
    dh = d_model // 2
    dq = d_model // 4
    toks = cc.shape[0]
    msg = TP * CAP
    right = lax.rem(x + 1, TP)
    left = lax.rem(x + TP - 1, TP)
    z = lax.div(s, groups)
    g = lax.rem(s, groups)

    def sp_ahead(dz, dg):
        return lax.rem(z + dz, zs) * groups + lax.rem(g + dg, groups)

    def sp_behind(dz, dg):
        return lax.rem(z + zs - dz, zs) * groups + lax.rem(g + groups - dg, groups)

    order = sorted(range(2, zs - 1), key=lambda dz: (min(dz, zs - dz) != 3, min(dz, zs - dz)))

    def zone(i):
        dz = order[0]
        for n, other in enumerate(order[1:]):
            dz = jnp.where(i == n + 1, other, dz)
        return dz

    def near_zone(k):
        return jnp.where(k == 0, 1, jnp.where(k == 1, zs - 1, 0))

    pairs = (
        (cc_h, cc), (cx_h, cx), (cb_h, cb), (ow_h, ow), (resid_h, resid),
        (sg_h, sg), (su_h, su), (sd_h, sd), (wg_h.at[0], wg), (wu_h.at[0], wu), (wd_h.at[0], wd),
    )
    loads = [pltpu.make_async_copy(a, b, load_sem.at[i]) for i, (a, b) in enumerate(pairs)]
    for one in loads:
        one.start()

    barrier = pltpu.get_barrier_semaphore()

    def tell(sem, sp, tp):
        pl.semaphore_signal(
            sem, inc=1, device_id=(sp, tp), device_id_type=pl.DeviceIdType.MESH
        )

    core = z * groups + g + 1 - 2 * lax.rem(g, 2)
    y_sides = (sp_ahead(0, 2), sp_behind(0, 2)) if groups > 2 else ()
    z_sides = (sp_ahead(1, 0), sp_behind(1, 0))
    ring_sides = (lax.rem(s + 1, sp_count), lax.rem(s + sp_count - 1, sp_count))
    for side in (right, left):
        tell(barrier, s, side)
    for side in ring_sides + (core,) + y_sides + z_sides:
        tell(barrier, side, x)
    n_near = 2 + 3 + len(y_sides) + 2
    rounds = [(core,)] + [y_sides] * (groups // 4) + [z_sides] * (zs // 2)

    def pass_on(k):
        if k < len(rounds):
            for side in rounds[k]:
                tell(known.at[k], side, x)

    def learn(k):
        if k < len(rounds):
            pl.semaphore_wait(known.at[k], len(rounds[k]))

    for i in range(3):
        loads[i].wait()
    prod[0:8] = jnp.zeros((8, prod.shape[1]), F32)
    prod[8 : 8 + toks] = cc[...].astype(F32) * cx[...].astype(F32)
    halo[...] = prod[toks : toks + 8]

    def mix(n):
        conv = prod[6 : 6 + n] * taps[0:1].astype(F32)
        conv = conv + prod[7 : 7 + n] * taps[1:2].astype(F32)
        conv = conv + prod[8 : 8 + n] * taps[2:3].astype(F32)
        mixed[0:n] = (cb[0:n].astype(F32) * conv).astype(BF16)

    def project(j):
        block = lax.rem(x + TP - j, TP)
        return mixed[pl.ds(pl.multiple_of(block * q, 16), q)]

    mix(toks)
    loads[3].wait()
    for n in range(4):
        for j in (2, 3, 1):
            proj[n // 2, j, n % 2] = jnp.dot(
                project(j), ow[:, n * dq : (n + 1) * dq], preferred_element_type=F32
            ).astype(BF16)

    pl.semaphore_wait(barrier, n_near)
    pass_on(0)
    halo_copy = remote(
        halo, halo_in, halo_sem.at[0], halo_sem.at[1], lax.rem(s + 1, sp_count), x
    )
    halo_copy.start()

    def ring_sum(b, b1, b2, ssem, rsem):
        def far_side():
            remote(b.at[2, 0], b1.at[0], ssem, rsem(0), s, right).start()
            remote(b.at[2, 1], b1.at[1], ssem, rsem(1), s, left).start()

        def to_right():
            remote(b.at[3, 1], b2.at[0, 1], ssem, rsem(2), s, right).start()

        def to_left():
            remote(b.at[1, 0], b2.at[1, 0], ssem, rsem(3), s, left).start()

        def begin():
            far_side()
            to_right()
            to_left()

        def turn():
            remote(b.at[2, 0], b1.at[0], ssem, rsem(0), s, left).wait_recv()
            add_into(b.at[3, 0], b1.at[0])
            remote(b.at[3, 0], b2.at[0, 0], ssem, rsem(4), s, right).start()
            remote(b.at[2, 1], b1.at[1], ssem, rsem(1), s, right).wait_recv()
            add_into(b.at[1, 1], b1.at[1])
            remote(b.at[1, 1], b2.at[1, 1], ssem, rsem(5), s, left).start()

        def finish():
            remote(b.at[3, 1], b2.at[0, 1], ssem, rsem(2), s, left).wait_recv()
            remote(b.at[1, 0], b2.at[1, 0], ssem, rsem(3), s, right).wait_recv()
            remote(b.at[3, 0], b2.at[0, 0], ssem, rsem(4), s, left).wait_recv()
            remote(b.at[1, 1], b2.at[1, 1], ssem, rsem(5), s, right).wait_recv()

        def drain():
            remote(b.at[0:3], b.at[0:3], ssem, rsem(0), s, right).wait_send()

        return begin, turn, finish, drain, (far_side, to_right, to_left)

    def ring_gather(b, ssem, rsem):
        def begin():
            remote(b.at[0], b.at[1], ssem, rsem(0), s, right).start()
            remote(b.at[0], b.at[3], ssem, rsem(1), s, left).start()

        def turn():
            remote(b.at[0], b.at[1], ssem, rsem(0), s, left).wait_recv()
            remote(b.at[1, 0], b.at[2, 0], ssem, rsem(2), s, right).start()
            remote(b.at[0], b.at[3], ssem, rsem(1), s, right).wait_recv()
            remote(b.at[3, 1], b.at[2, 1], ssem, rsem(3), s, left).start()

        def finish():
            remote(b.at[1, 0], b.at[2, 0], ssem, rsem(2), s, left).wait_recv()
            remote(b.at[3, 1], b.at[2, 1], ssem, rsem(3), s, right).wait_recv()

        def drain():
            remote(b.at[0:3], b.at[0:3], ssem, rsem(0), s, right).wait_send()

        return begin, turn, finish, drain

    sums = [
        ring_sum(
            proj.at[c], proj1.at[c], proj2.at[c], proj_s.at[c], lambda k, c=c: proj_r.at[c, k]
        )
        for c in range(2)
    ]
    gathers = [
        ring_gather(raw.at[c], nrm_s.at[c], lambda k, c=c: nrm_r.at[c, k]) for c in range(2)
    ]

    for c in range(2):
        pl.when(x != 2)(sums[c][4][0])
        pl.when(x < 2)(sums[c][4][1])
        pl.when((x == 0) | (x == 3))(sums[c][4][2])

    learn(0)
    pass_on(1)
    halo_copy.wait_recv()
    prod[0:8] = halo_in[...] * jnp.where(s == 0, 0.0, 1.0)
    mix(16)
    for n in range(4):
        proj[n // 2, x, n % 2, 0:16] = jnp.dot(
            mixed[0:16], ow[:, n * dq : (n + 1) * dq], preferred_element_type=F32
        ).astype(BF16)
    for c in range(2):
        pl.when(x == 2)(sums[c][4][0])
        pl.when(x >= 2)(sums[c][4][1])
        pl.when((x == 1) | (x == 2))(sums[c][4][2])
    learn(1)
    pass_on(2)
    for n in range(4):
        own[n // 2, n % 2] = jnp.dot(
            project(0), ow[:, n * dq : (n + 1) * dq], preferred_element_type=F32
        )
    learn(2)
    pass_on(3)

    rowform[0:2] = routes[...].astype(F32)
    rowform[2:4] = rweight[...]
    colform[...] = rowform[...].T
    before = lax.broadcasted_iota(jnp.int32, (q, q), 0) > lax.broadcasted_iota(
        jnp.int32, (q, q), 1
    )
    earlier = jnp.where(before, 1.0, 0.0).astype(BF16)

    def table(j, dz, dg, rank, extra):
        expert = lax.rem(dz + z, zs) * groups + lax.rem(dg + g, groups)
        expert = expert.astype(F32)
        rows = pl.ds(pl.multiple_of(lax.rem(x + TP - j, TP) * q, 16), q)
        is_0 = expert == colform[rows, 0:1]
        named = jnp.where(is_0 | (expert == colform[rows, 1:2]), 1.0, 0.0)
        count = jnp.dot(earlier, named.astype(BF16), preferred_element_type=F32)
        held = jnp.where((count == rank.astype(F32)) & extra, named, 0.0)
        weight = jnp.where(is_0, colform[rows, 2:3], colform[rows, 3:4]) * held
        high = weight.astype(BF16)
        return held.T.astype(BF16), high, (weight - high.astype(F32)).astype(BF16)

    far_slots = far * groups * CAP
    i_slot = lax.broadcasted_iota(jnp.int32, (q, far_slots), 1)
    offset = lax.div(i_slot, CAP)
    disp[...], wcomb[0:q], wcomb[q : 2 * q] = table(
        0, zone(lax.div(offset, groups)), lax.rem(offset, groups), lax.rem(i_slot, CAP),
        i_slot >= 0,
    )

    learn(3)
    pass_on(4)
    sums[0][1]()
    sums[1][1]()

    def settle(c):
        sums[c][2]()
        for h in range(2):
            n = 2 * c + h
            total = own[c, h] + proj2[c, 0, h].astype(F32) + proj2[c, 1, h].astype(F32)
            total = total + resid[:, n * dq : (n + 1) * dq].astype(F32)
            raw[c, 0, h] = total.astype(BF16)
        gathers[c][0]()

    def normalize(j):
        square = jnp.zeros((q, 1), F32)
        for n in range(4):
            m = raw[n // 2, j, n % 2].astype(F32)
            square = square + jnp.sum(m * m, axis=-1, keepdims=True)
        scale = lax.rsqrt(square * (1.0 / d_model) + 1e-06)
        for n in range(4):
            m = raw[n // 2, j, n % 2].astype(F32)
            nrm[n, j] = (m * scale * gain[:, n * dq : (n + 1) * dq]).astype(BF16)

    near_slots = NEAR * groups * msg
    n_slot = lax.broadcasted_iota(jnp.int32, (q, near_slots), 1)
    near_offset = lax.div(n_slot, msg)
    b_slot = lax.broadcasted_iota(jnp.int32, (q, NEAR * groups * CAP), 1)
    b_offset = lax.div(b_slot, CAP)
    for j in range(TP):
        high, low = pl.ds(2 * j * q, q), pl.ds((2 * j + 1) * q, q)
        _, near_w[high], near_w[low] = table(
            j, near_zone(lax.div(near_offset, groups)), lax.rem(near_offset, groups),
            lax.rem(n_slot, CAP), lax.rem(lax.div(n_slot, CAP), TP) == j,
        )
        near_disp[j], _, _ = table(
            j, near_zone(lax.div(b_offset, groups)), lax.rem(b_offset, groups),
            lax.rem(b_slot, CAP), b_slot >= 0,
        )
        learn(4 + j)
        pass_on(5 + j)
        if j == 1:
            loads[4].wait()
            settle(0)

    settle(1)
    normalize(0)

    zone_rows = groups * CAP

    def far_dispatch(low, high):
        @pl.loop(low, high)
        def _(i):
            rows = disp[pl.ds(pl.multiple_of(i * zone_rows, zone_rows), zone_rows)]
            for n in range(4):
                picked = jnp.dot(rows, nrm[n, 0], preferred_element_type=F32)
                outgoing[i, :, :, :, n * dq : (n + 1) * dq] = picked.astype(BF16).reshape(
                    2, half, CAP, dq
                )
            for dg in range(groups):
                remote(
                    outgoing.at[i, dg // half, dg % half], arr.at[i, 0, dg // half, dg % half],
                    a2a_s.at[i], a2a_r.at[i], sp_ahead(zone(i), dg), x,
                ).start()

    near_rows = groups * msg

    def near_dispatch(j):
        for n in range(4):
            picked = jnp.dot(near_disp[j], nrm[n, j], preferred_element_type=F32)
            near_out[:, :, j, :, n * dq : (n + 1) * dq] = picked.astype(BF16).reshape(
                NEAR, groups, CAP, dq
            )

        @pl.loop(0, NEAR)
        def _(k):
            for dg in range(groups):
                @pl.when((k != NEAR - 1) | (dg != 0))
                def _():
                    remote(
                        near_out.at[k, dg, j], near_arr.at[k, dg, j], out_s.at[k], out_r.at[k],
                        sp_ahead(near_zone(k), dg), x,
                    ).start()

    later = min(3, far)
    far_dispatch(0, later)
    near_dispatch(0)
    for one in loads[5:]:
        one.wait()
    gathers[0][1]()
    gathers[1][1]()
    normalize(1)
    normalize(3)
    far_dispatch(later, far)
    near_dispatch(1)
    near_dispatch(3)

    def near_send(src, dst, k, ssem, rsem, target):
        for dg in range(groups):
            @pl.when((k != NEAR - 1) | (dg != 0))
            def _():
                rows = slice(dg * msg, (dg + 1) * msg)
                remote(
                    src.at[k, rows], dst.at[k, rows], ssem.at[k], rsem.at[k],
                    target(near_zone(k), dg), x,
                ).start()

    def near_wait(k, ssem, rsem, recv):
        def fire(a):
            one = remote(a, a, ssem.at[k], rsem.at[k], s, right)
            if recv:
                one.wait_recv()
            else:
                one.wait_send()

        @pl.when(k != NEAR - 1)
        def _():
            fire(near_res.at[k])

        @pl.when(k == NEAR - 1)
        def _():
            fire(near_res.at[k, msg:near_rows])

    def chain(i):
        return ring_sum(res.at[i], res1.at[i], res2.at[i], rs_s.at[i], lambda k: rs_r.at[i, k])

    def spread(i):
        return ring_gather(arr.at[i], ag_s.at[i], lambda k: ag_r.at[i, k])

    n_rows = TP * groups * CAP
    kc = min(256, d_model)
    nc = dq

    def expert(read, write):
        gate = jnp.zeros((n_rows, wg.shape[1]), F32)
        up = jnp.zeros((n_rows, wg.shape[1]), F32)
        for k in range(d_model // kc):
            cols = slice(k * kc, (k + 1) * kc)
            block = read(cols)
            gate = gate + jnp.dot(block, wg[cols], preferred_element_type=F32)
            up = up + jnp.dot(block, wu[cols], preferred_element_type=F32)
        hidden = (jax.nn.silu(gate) * up).astype(BF16)
        for n in range(d_model // nc):
            cols = slice(n * nc, (n + 1) * nc)
            write(cols, jnp.dot(hidden, wd[:, cols], preferred_element_type=F32).astype(BF16))

    def far_expert(i):
        def write(cols, value):
            res[i, :, :, :, :, cols] = value.reshape(TP, 2, half, CAP, nc)

        expert(lambda cols: arr[i, :, :, :, :, cols].reshape(n_rows, kc), write)

    def near_expert(k):
        def write(cols, value):
            near_res[k, :, cols] = value

        expert(lambda cols: near_arr[k, :, :, :, cols].reshape(n_rows, kc), write)

    _, part_turn, part_finish, part_drain, (part_far, part_right, part_left) = ring_sum(
        part, part1, part2, part_s, lambda k: part_r.at[k]
    )

    def shared():
        gate = jnp.zeros((TP * q, sg.shape[1]), F32)
        up = jnp.zeros((TP * q, sg.shape[1]), F32)
        for n in range(4):
            block = nrm[n].reshape(TP * q, dq)
            gate = gate + jnp.dot(block, sg[n * dq : (n + 1) * dq], preferred_element_type=F32)
            up = up + jnp.dot(block, su[n * dq : (n + 1) * dq], preferred_element_type=F32)
        hidden = (jax.nn.silu(gate) * up).astype(BF16)
        for h in range(2):
            partf[:, h] = jnp.dot(
                hidden, sd[:, h * dh : (h + 1) * dh], preferred_element_type=F32
            ).reshape(TP, q, dh)

    def near_combine(j):
        weights = near_w[2 * j * q : 2 * (j + 1) * q]
        for n in range(d_model // nc):
            h, c = divmod(n * nc, dh)
            block = near_ret[:, :, n * nc : (n + 1) * nc].reshape(near_slots, nc)
            both = jnp.dot(weights, block, preferred_element_type=F32)
            total = partf[j, h, :, c : c + nc] + both[:q] + both[q:]
            part[j, h, :, c : c + nc] = total.astype(BF16)

    def far_combine():
        for n in range(d_model // nc):
            h, c = divmod(n * nc, dh)
            block = ret[:, :, :, :, n * nc : (n + 1) * nc].reshape(far_slots, nc)
            both = jnp.dot(wcomb[...], block, preferred_element_type=F32)
            own[n // 2, n % 2] = (
                both[:q] + both[q:] + raw[n // 2, 0, n % 2].astype(F32)
                + part[0, h, :, c : c + nc].astype(F32)
            )

    @pl.loop(0, far + 4)
    def _(i):
        @pl.when(i < far)
        def _():
            a = arr.at[i, 0]
            remote(a, a, a2a_s.at[i], a2a_r.at[i], s, right).wait_recv()
            spread(i)[0]()

        @pl.when(i == NEAR_STEP)
        def _():
            @pl.loop(0, NEAR)
            def _(k):
                near_wait(k, out_s, out_r, True)
                near_expert(k)
                near_send(near_res, near_ret, k, home_s, home_r, sp_behind)

        @pl.when(i == 0)
        def _():
            gathers[0][2]()
            gathers[1][2]()
            normalize(2)
            near_dispatch(2)
            near_arr[NEAR - 1, 0] = near_out[NEAR - 1, 0]

        @pl.when((i >= 1) & (i < far + 1))
        def _():
            spread(i - 1)[1]()

        @pl.when(i == 1)
        def _():
            shared()

        @pl.when((i >= 2) & (i < far + 2))
        def _():
            spread(i - 2)[2]()
            far_expert(i - 2)
            chain(i - 2)[0]()

        @pl.when((i >= 3) & (i < far + 3))
        def _():
            chain(i - 3)[1]()

        @pl.when(i == far + 3)
        def _():
            near_ret[NEAR - 1, 0:msg] = near_res[NEAR - 1, 0:msg]
            for k in range(NEAR):
                near_wait(k, home_s, home_r, True)
            near_combine(2)
            part_far()

        @pl.when((i >= 4) & (i < far + 4))
        def _():
            k = i - 4
            chain(k)[2]()
            summed[k] = (
                res[k, 0].astype(F32) + res2[k, 0].astype(F32) + res2[k, 1].astype(F32)
            ).astype(BF16)
            for dg in range(groups):
                remote(
                    summed.at[k, dg // half, dg % half], ret.at[k, dg // half, dg % half],
                    back_s.at[k], back_r.at[k], sp_behind(zone(k), dg), x,
                ).start()

    near_combine(3)
    part_right()
    near_combine(1)
    part_left()
    near_combine(0)
    part_turn()
    halo_copy.wait_send()
    for c in range(2):
        sums[c][3]()
        gathers[c][3]()

    @pl.loop(0, far)
    def _(i):
        a = outgoing.at[i]
        remote(a, a, a2a_s.at[i], a2a_r.at[i], s, right).wait_send()
        b = summed.at[i]
        remote(b, b, back_s.at[i], back_r.at[i], s, right).wait_send()
        spread(i)[3]()
        chain(i)[3]()

    for k in range(NEAR):
        near_wait(k, out_s, out_r, False)
        near_wait(k, home_s, home_r, False)

    @pl.loop(0, far)
    def _(i):
        a = ret.at[i]
        remote(a, a, back_s.at[i], back_r.at[i], s, right).wait_recv()

    far_combine()
    part_finish()
    for n in range(4):
        h, c = divmod(n * dq, dh)
        total = own[n // 2, n % 2] + part2[0, h, :, c : c + dq].astype(F32)
        total = total + part2[1, h, :, c : c + dq].astype(F32)
        out[:, n * dq : (n + 1) * dq] = total.astype(BF16)
    part_drain()


def local(
    resid, conv_b, conv_c, conv_x, conv_taps, out_weight, norm_gain, routes, route_weight,
    expert_gate, expert_up, expert_down, shared_gate, shared_up, shared_down,
):
    sp_count = lax.axis_size("sp")
    groups = max(2, sp_count // 8)
    zs = sp_count // groups
    half = groups // 2
    far = zs - NEAR
    near_slots = NEAR * groups * TP * CAP
    q, d = resid.shape
    toks, ch = conv_b.shape
    ff = expert_gate.shape[2]
    dh = d // 2
    dq = d // 4
    vmem = pltpu.VMEM
    dma = pltpu.SemaphoreType.DMA
    anywhere = pl.BlockSpec(memory_space=pl.ANY)
    inside = pl.BlockSpec(memory_space=pltpu.VMEM)
    return pl.pallas_call(
        functools.partial(kernel, groups),
        out_shape=pltpu.VMEM((q, d), BF16),
        in_specs=[anywhere] * 4 + [inside, anywhere] + [inside] * 3 + [anywhere] * 6,
        out_specs=inside,
        scratch_shapes=[
            vmem((q, d), BF16), vmem((toks, ch), BF16), vmem((toks, ch), BF16),
            vmem((toks, ch), BF16), vmem((ch, d), BF16),
            vmem((d, ff), BF16), vmem((d, ff), BF16), vmem((ff, d), BF16),
            vmem((d, ff), BF16), vmem((d, ff), BF16), vmem((ff, d), BF16),
            vmem((toks + 8, ch), F32), vmem((toks, ch), BF16), vmem((8, ch), F32), vmem((8, ch), F32),
            vmem((2, 2, q, dq), F32),
            vmem((2, 4, 2, q, dq), BF16), vmem((2, 2, q, dq), BF16),
            vmem((2, 2, 2, q, dq), BF16),
            vmem((2, 4, 2, q, dq), BF16), vmem((4, 4, q, dq), BF16),
            vmem((4, 2, q, dh), BF16), vmem((2, q, dh), BF16), vmem((2, 2, q, dh), BF16),
            vmem((4, 2, q, dh), F32),
            vmem((8, toks), F32), vmem((toks, 8), F32),
            vmem((far * groups * CAP, q), BF16), vmem((2 * q, far * groups * CAP), BF16),
            vmem((far, 2, half, CAP, d), BF16),
            vmem((far, 4, 2, half, CAP, d), BF16),
            vmem((far, 4, 2, half, CAP, d), BF16),
            vmem((far, 2, half, CAP, d), BF16),
            vmem((far, 2, 2, half, CAP, d), BF16),
            vmem((far, 2, half, CAP, d), BF16),
            vmem((far, 2, half, CAP, d), BF16),
            vmem((TP, NEAR * groups * CAP, q), BF16), vmem((2 * TP * q, near_slots), BF16),
            vmem((NEAR, groups, TP, CAP, d), BF16), vmem((NEAR, groups, TP, CAP, d), BF16),
            vmem((NEAR, groups * TP * CAP, d), BF16), vmem((NEAR, groups * TP * CAP, d), BF16),
            dma((11,)), dma((2,)), dma((2,)), dma((2, 6)), dma((2,)), dma((2, 4)), dma(()), dma((6,)),
            dma((far,)), dma((far,)), dma((far,)), dma((far, 4)), dma((far,)), dma((far, 6)),
            dma((far,)), dma((far,)), dma((NEAR,)), dma((NEAR,)), dma((NEAR,)), dma((NEAR,)),
            pltpu.SemaphoreType.REGULAR((8,)),
        ],
        compiler_params=pltpu.CompilerParams(
            collective_id=0, has_side_effects=True, vmem_limit_bytes=60 * 1024 * 1024
        ),
        name="layer",
    )(
        resid, conv_b, conv_c, conv_x, conv_taps, out_weight, norm_gain.reshape(1, d), routes.T,
        route_weight.T, expert_gate, expert_up, expert_down, shared_gate, shared_up, shared_down,
    )


def solution(mesh):
    return jax.shard_map(
        local,
        mesh=mesh,
        in_specs=(
            P(("sp", "tp"), None),
            P("sp", "tp"),
            P("sp", "tp"),
            P("sp", "tp"),
            P(None, "tp"),
            P("tp", None),
            P(),
            P("sp", None),
            P("sp", None),
            P("sp", None, "tp"),
            P("sp", None, "tp"),
            P("sp", "tp", None),
            P(None, "tp"),
            P(None, "tp"),
            P("tp", None),
        ),
        out_specs=P(("sp", "tp"), None),
        check_vma=False,
    )
```
